256 devices in a mesh: grp: 2 (over y), sp: 16 (over z), tp: 8 (over x, core).
Axes of the slice: x: 4, y: 2, z: 16, core: 2. Of those that a mesh axis runs over, the one named last changes fastest.
The devices are a block of a 4x16x16 slice.
Arguments:
- tokens: bfloat16 [32, 4096, 4096], P(('grp', 'tp'), 'sp'), parts along dimension 0, may hold values from -8 to 8, as said below
- offsets: int32 [32], P(('grp', 'tp')), parts along dimension 0, may hold values from 0 to 4095
- in_gain: float32 [4096], replicated, may hold values from 0.1 to 1.9
- w_latent: bfloat16 [4096, 1024], P('sp'), may hold values from -0.09375 to 0.09375
- w_rope_key: bfloat16 [4096, 32], replicated, may hold values from -0.09375 to 0.09375
- kv_gain: float32 [1024], replicated, may hold values from 0.1 to 1.9
- w_up_key: bfloat16 [1024, 2048], P(None, 'tp'), may hold values from -0.1875 to 0.1875
- w_up_value: bfloat16 [1024, 2048], P(None, 'tp'), may hold values from -0.1875 to 0.1875
- q_nope: bfloat16 [32, 2048], P(('grp', 'sp'), 'tp'), parts along dimension 0, may hold values from -300 to 300, as said below
- q_rope: bfloat16 [32, 1024], P(('grp', 'sp'), 'tp'), parts along dimension 0, may hold values from -16 to 16
Outputs:
- keys: bfloat16 [32, 4096, 2048], P(('grp', 'sp'), None, 'tp'), parts along dimension 0
- values: bfloat16 [32, 4096, 2048], P(('grp', 'sp'), None, 'tp'), parts along dimension 0
- rope_keys: bfloat16 [32, 32, 4096], P(('grp', 'sp')), parts along dimension 0
- read: bfloat16 [32, 2048], P(('grp', 'sp'), 'tp'), parts along dimension 0
The draws below stay inside these ranges and needn't reach their ends.
There are 2 independent parts, one for each index of `grp`. The reference program is written for one: setup_inputs(seed, part) draws one part's arguments, and reference() takes and returns one part's arrays. A program takes and returns all parts, laid end to end along the dimension named above; an argument that names none is the same for every part. Nothing has to cross between parts.
Inputs may be any that keep to these rules, and one draw needn't show every extreme that they name: `tokens`: entries of the layer's input. `q_nope`: entries of the first decoding token's queries.
All inputs are finite; a program needn't handle non-finite values.
Results may differ from the reference program's by a relative error of at most 0.02.
Values may be sent and summed in bfloat16 or wider, within the bound.
A program may use at most 128 MiB of HBM per device.

```python
import jax
import jax.numpy as jnp
from jax import lax

D = 4096
HEADS = 32
HEAD = 64
ROPE = 32
KV_RANK = 1024
SEQS = 16
LEN = 4096


def draw_tokens(key, part):
    first, second = jax.random.split(jax.random.fold_in(key, 29))
    noise = jax.random.normal(first, (SEQS, LEN, D), jnp.float32)
    base = jnp.clip(noise, -6.0, 6.0)
    return base.astype(jnp.bfloat16)


def draw_q_nope(key, part):
    first, second = jax.random.split(jax.random.fold_in(key, 17))
    base = jax.random.normal(first, (SEQS, HEADS, HEAD), jnp.float32) * 4.0
    base = jnp.clip(base, -16.0, 16.0)
    return base.reshape(SEQS, HEADS * HEAD).astype(jnp.bfloat16)


def plant(array, key, low, largest):
    place = [jax.random.randint(jax.random.fold_in(key, axis), (), 0, length) for axis, length in enumerate(array.shape)]
    widest = array.shape.index(max(array.shape))
    neighbour = place[:widest] + [(place[widest] + 1) % array.shape[widest]] + place[widest + 1:]
    return array.at[tuple(place)].set(low).at[tuple(neighbour)].set(largest)


def block_levels(stream_key, extent, pieces, low, top_value):
    loudness = 1.0
    for dim, parts in pieces:
        steps = jax.random.uniform(jax.random.fold_in(jax.random.fold_in(stream_key, 6), dim), (parts,), jnp.float32, low / len(pieces), top_value / len(pieces))
        loudness = loudness * jnp.repeat(jnp.exp(steps), extent[dim] // parts).reshape((-1,) + (1,) * (len(extent) - 1 - dim))
    return loudness


def normal_values(key, extent, deviation, reach, shards=(), kind=jnp.bfloat16):
    drawn = deviation * jax.random.normal(key, extent, jnp.float32)
    if shards:
        drawn = drawn * block_levels(key, extent, shards, -0.22, 0.18)
    return jnp.clip(drawn, -reach, reach).astype(kind)


def setup_inputs(seed: int = 0, part: int = 0) -> dict:
    key_list = jax.random.split(jax.random.key(seed), 11)
    own_keys = jax.random.split(jax.random.fold_in(key_list[10], part), 11)
    return {
        "tokens": draw_tokens(jax.random.fold_in(jax.random.fold_in(key_list[10], part), 71), part),
        "offsets": plant(jax.random.randint(own_keys[1], (SEQS,), 0, 4096), jax.random.fold_in(own_keys[1], 1), 0, 4095).astype(jnp.int32),
        "in_gain": jnp.clip(1.0 + 0.18 * jax.random.normal(key_list[2], (D,), jnp.float32), 0.1, 1.9),
        "w_latent": normal_values(key_list[3], (D, KV_RANK), D ** -0.5, 0.09375, ((0, 16),)),
        "w_rope_key": normal_values(key_list[4], (D, ROPE), D ** -0.5, 0.09375),
        "kv_gain": jnp.clip(1.0 + 0.18 * jax.random.normal(key_list[5], (KV_RANK,), jnp.float32), 0.1, 1.9),
        "w_up_key": normal_values(key_list[6], (KV_RANK, HEADS * HEAD), KV_RANK ** -0.5, 0.1875, ((1, 8),)),
        "w_up_value": normal_values(key_list[7], (KV_RANK, HEADS * HEAD), KV_RANK ** -0.5, 0.1875, ((1, 8),)),
        "q_nope": draw_q_nope(jax.random.fold_in(jax.random.fold_in(key_list[10], part), 71), part),
        "q_rope": normal_values(own_keys[9], (SEQS, HEADS * ROPE), 4.0, 16.0, ((0, 16), (1, 8))),
    }


EPS = 1e-06

def rms_scale(values, gain):
    wide = values.astype(jnp.float32)
    return wide * lax.rsqrt(lax.optimization_barrier(jnp.mean(wide * wide, axis=-1, keepdims=True)) + EPS) * gain.astype(jnp.float32)

def rotate(raw, position):
    inverse = 10000.0 ** (-jnp.arange(0, ROPE, 2).astype(jnp.float32) / ROPE)
    angle = position.astype(jnp.float32)[:, None] * inverse[None, :]
    cosine, sine = (jnp.cos(angle), jnp.sin(angle))
    half = ROPE // 2
    first, second = (raw[:, :half], raw[:, half:])
    return jnp.concatenate([first * cosine - second * sine, second * cosine + first * sine], axis=-1)

def reference(tokens, offsets, in_gain, w_latent, w_rope_key, kv_gain, w_up_key, w_up_value, q_nope, q_rope):

    def one_prompt(args):
        prompt, start = args
        normed = rms_scale(prompt, in_gain).astype(jnp.bfloat16)
        latent_raw = jnp.dot(normed, w_latent, preferred_element_type=jnp.float32)
        latent = rms_scale(latent_raw, kv_gain).astype(jnp.bfloat16)
        rope_raw = jnp.dot(normed, w_rope_key, preferred_element_type=jnp.float32)
        position = start + jnp.arange(LEN, dtype=jnp.int32)
        rotated = rotate(rope_raw, position).astype(jnp.bfloat16)
        keys = jnp.dot(latent, w_up_key, preferred_element_type=jnp.float32).astype(jnp.bfloat16)
        values = jnp.dot(latent, w_up_value, preferred_element_type=jnp.float32).astype(jnp.bfloat16)
        return (keys, values, rotated.T)
    keys, values, rope_keys = lax.map(one_prompt, (tokens, offsets))
    query = q_nope.astype(jnp.float32).reshape(SEQS, HEADS, HEAD)
    rotary_q = q_rope.astype(jnp.float32).reshape(SEQS, HEADS, ROPE)
    keys_wide = keys.astype(jnp.float32).reshape(SEQS, LEN, HEADS, HEAD)
    scores = jnp.einsum('shd,sjhd->shj', query, keys_wide)
    scores = scores + jnp.einsum('shr,srj->shj', rotary_q, rope_keys.astype(jnp.float32))
    scores = scores / jnp.sqrt(jnp.float32(HEAD + ROPE))
    weights = jax.nn.softmax(scores, axis=-1).astype(jnp.bfloat16)
    values_wide = values.astype(jnp.float32).reshape(SEQS, LEN, HEADS, HEAD)
    read = jnp.einsum('shj,sjhd->shd', weights.astype(jnp.float32), values_wide)
    read = read.astype(jnp.bfloat16).reshape(SEQS, HEADS * HEAD)
    return (keys, values, rope_keys, read)
```

```python
import functools

import jax
import jax.numpy as jnp
from jax import lax
from jax.experimental import pallas as pl
from jax.experimental.pallas import tpu as pltpu
from jax.sharding import PartitionSpec as P

HEAD = 64
ROPE = 32
EPS = 1e-06
MESH = pl.DeviceIdType.MESH
FULL = 48

DO_W = True
DO_L = True
DO_C = True


def exchange(
    n_sp, n_tp, tok_hbm, off_ref, gain_ref, wl_hbm, wrope_ref, kvg_ref, wk_hbm, wv_hbm,
    keys_ref, values_ref, rope_ref,
    norm, wfull, wup, lat, acc, latall, ropeown,
    local_sem, wz_sem, wx_sem, wp_sem, wsend, dir_sem, lx_sem, lp_sem, lsend, rsem, rsend,
):
    z = lax.axis_index("sp")
    t = lax.axis_index("tp")
    n_x = n_tp // 2
    x, c = t // 2, lax.rem(t, 2)
    rows = norm.shape[0] // 2
    width = norm.shape[1]
    rank = lat.shape[1]
    depth = width // n_sp
    half = depth // 2
    quarter = rank // n_x
    piece = rows // n_x
    heads = keys_ref.shape[1]

    def wrap(v, n):
        return lax.rem(v + 2 * n, n)

    def dev(xx, cc, zz):
        return {"sp": zz, "tp": 2 * xx + cc}

    z_next, z_prev = wrap(z + 1, n_sp), wrap(z - 1, n_sp)
    right = dev(wrap(x + 1, n_x), c, z)
    left = dev(wrap(x - 1, n_x), c, z)
    up = dev(x, c, z_next)
    down = dev(x, c, z_prev)
    partner = dev(x, 1 - c, z)
    home = lax.rem(z, 2)
    has_self = jnp.logical_and(t == z // 2, c == home)

    loads = [
        pltpu.make_async_copy(wl_hbm, wfull.at[pl.ds(z * depth, depth)], local_sem.at[0]),
        pltpu.make_async_copy(tok_hbm, norm, local_sem.at[1]),
        pltpu.make_async_copy(wk_hbm, wup.at[:, pl.ds(0, heads)], local_sem.at[2]),
        pltpu.make_async_copy(wv_hbm, wup.at[:, pl.ds(heads, heads)], local_sem.at[3]),
    ]
    for load in loads:
        load.start()

    barrier = pltpu.get_barrier_semaphore()

    def greet(device):
        pl.semaphore_signal(barrier, inc=1, device_id=device, device_id_type=MESH)

    for dx in range(n_x):
        for dc in range(2):
            if dx or dc:
                greet(dev(wrap(x + dx, n_x), lax.rem(c + dc, 2), z))
    greet(up)
    greet(down)
    dests = [(j, q) for j in range(2) for q in range(n_x)]
    src_x, src_c = z // 4, lax.rem(z // 2, 2)
    for j, q in dests:
        own = jnp.logical_and(has_self, jnp.logical_and(2 * t + j == z, x == q))
        pl.when(jnp.logical_not(own))(functools.partial(greet, dev(jnp.int32(q), home, 2 * t + j)))
    for i in range(n_sp // 2):
        own = jnp.logical_and(has_self, 2 * i + c == z)
        pl.when(jnp.logical_not(own))(functools.partial(greet, dev(src_x, src_c, 2 * i + c)))
    pl.semaphore_wait(barrier, 2 * n_x - 1 + 2 + 2 * n_x + n_sp // 2 - 2 * has_self.astype(jnp.int32))

    def send(src, dst, device, send_sem, recv_sem):
        pltpu.make_async_remote_copy(
            src_ref=src, dst_ref=dst, send_sem=send_sem, recv_sem=recv_sem,
            device_id=device, device_id_type=MESH,
        ).start()

    def arrived(dst, recv_sem):
        pltpu.make_async_copy(dst, dst, recv_sem).wait()

    def w_full(s):
        return wfull.at[pl.ds(s * depth + c * half, FULL)]

    def w_part(s, xx):
        return wfull.at[
            pl.ds(s * depth + c * half + FULL, half - FULL), pl.ds(pl.multiple_of(xx * quarter, quarter), quarter)
        ]

    def w_half(s, cc):
        return wfull.at[pl.ds(s * depth + cc * half, half)]

    steps = n_sp // 2
    limit = {("f", 1): steps, ("f", -1): steps - 1, ("q", 1): steps - 1, ("q", -1): steps}

    def z_send(kind, sign, k):
        s = wrap(z - sign * k, n_sp)
        ref = w_full(s) if kind == "f" else w_part(s, x)
        row = ("f", "q").index(kind) * 2 + (sign < 0)
        send(ref, ref, up if sign > 0 else down, wsend.at[row], wz_sem.at[row, k])

    def z_arrive(kind, sign, k):
        s = wrap(z - sign * k, n_sp)
        ref = w_full(s) if kind == "f" else w_part(s, x)
        row = ("f", "q").index(kind) * 2 + (sign < 0)
        arrived(ref, wz_sem.at[row, k - 1])
        if k < limit[kind, sign]:
            z_send(kind, sign, k)
        if kind == "q":
            col = k - 1 if sign > 0 else steps + k - 2
            send(ref, ref, right, wsend.at[4], wx_sem.at[0, col])
            send(ref, ref, left, wsend.at[5], wx_sem.at[1, col])

    def x_arrive(sign, k):
        s = wrap(z - sign * k, n_sp)
        col = k - 1 if sign > 0 else steps + k - 2
        from_left, from_right = w_part(s, wrap(x - 1, n_x)), w_part(s, wrap(x + 1, n_x))
        arrived(from_left, wx_sem.at[0, col])
        if sign > 0:
            send(from_left, from_left, right, wsend.at[6], wx_sem.at[2, col])
        arrived(from_right, wx_sem.at[1, col])
        if sign < 0:
            send(from_right, from_right, left, wsend.at[6], wx_sem.at[2, col])

    def far_arrive(sign, k):
        s = wrap(z - sign * k, n_sp)
        col = k - 1 if sign > 0 else steps + k - 2
        far = w_part(s, wrap(x + 2, n_x))
        arrived(far, wx_sem.at[2, col])
        ref = w_half(s, c)
        send(ref, ref, partner, wsend.at[7], wp_sem.at[col])

    loads[0].wait()
    if DO_W:
        for kind in ("f", "q"):
            for sign in (1, -1):
                z_send(kind, sign, 0)

    loads[1].wait()

    @pl.loop(0, 2 * rows // 16)
    def _(n):
        r = pl.ds(pl.multiple_of(n * 16, 16), 16)
        wide = norm[r, :].astype(jnp.float32)
        scale = lax.rsqrt(jnp.sum(wide * wide, axis=-1, keepdims=True) * (1.0 / width) + EPS)
        norm[r, :] = (wide * scale * gain_ref[...]).astype(jnp.bfloat16)

    raw = lax.dot_general(
        wrope_ref[...], norm[...], (((1,), (1,)), ((), ())), preferred_element_type=jnp.float32
    )
    index = lax.broadcasted_iota(jnp.int32, (ROPE // 2, rows), 0).astype(jnp.float32) * 2.0
    inverse = jnp.exp(index * (-jnp.log(jnp.float32(10000.0)) / ROPE))
    place = lax.broadcasted_iota(jnp.int32, (ROPE // 2, rows), 1)
    for j in range(2):
        angle = (off_ref[j] + z * rows + place).astype(jnp.float32) * inverse
        cosine, sine = jnp.cos(angle), jnp.sin(angle)
        first = raw[: ROPE // 2, j * rows:(j + 1) * rows]
        second = raw[ROPE // 2:, j * rows:(j + 1) * rows]
        ropeown[j] = jnp.concatenate(
            [first * cosine - second * sine, second * cosine + first * sine], axis=0
        ).astype(jnp.bfloat16)

    column = lax.rem(z // 2, n_x)
    for j in range(2):
        own = jnp.logical_and(has_self, jnp.logical_and(2 * t + j == z, x == column))
        dst = rope_ref.at[:, pl.ds(pl.multiple_of(z * rows, rows), rows)]

        @pl.when(own)
        def _():
            pltpu.make_async_copy(ropeown.at[j], dst, rsem.at[z]).start()

        @pl.when(jnp.logical_not(own))
        def _():
            send(ropeown.at[j], dst, dev(column, home, 2 * t + j), rsend.at[0, j], rsem.at[z])

    if DO_W:
        for k in range(1, steps + 1):
            for sign in (1, -1):
                for kind in ("q", "f"):
                    if k <= limit[kind, sign]:
                        z_arrive(kind, sign, k)
            for sign in (1, -1):
                if 1 <= k - 1 <= limit["q", sign]:
                    x_arrive(sign, k - 1)
            for sign in (1, -1):
                if 1 <= k - 2 <= limit["q", sign]:
                    far_arrive(sign, k - 2)
        x_arrive(-1, steps)
        for sign in (1, -1):
            far_arrive(sign, steps - 1)
        far_arrive(-1, steps)
        for sign in (1, -1):
            for k in range(1, limit["q", sign] + 1):
                col = k - 1 if sign > 0 else steps + k - 2
                arrived(w_half(wrap(z - sign * k, n_sp), 1 - c), wp_sem.at[col])

    def rope_block(s):
        return rope_ref.at[:, pl.ds(pl.multiple_of(s * rows, rows), rows)]

    peers = [(dx, dc) for dx in range(n_x) for dc in range(2) if dx or dc]
    for g in range(n_sp // 2 // n_x):
        s = 2 * (x + n_x * g) + c
        arrived(rope_block(s), rsem.at[s])
        for n, (dx, dc) in enumerate(peers):
            send(
                rope_block(s), rope_block(s), dev(wrap(x + dx, n_x), lax.rem(c + dc, 2), z),
                rsend.at[1 + g, n], rsem.at[s],
            )

    def own_piece(j, q):
        return lat.at[pl.ds(j * rows + q * piece, piece)]

    def place_of(s, q):
        return latall.at[pl.ds(pl.multiple_of(s * rows + q * piece, piece), piece)]

    for j in range(2):
        if DO_C:
            @pl.loop(0, n_x)
            def _(n):
                cols = pl.ds(pl.multiple_of(n * quarter, quarter), quarter)
                acc[:, cols] = jnp.dot(
                    norm[j * rows:(j + 1) * rows, :], wfull[:, cols], preferred_element_type=jnp.float32
                )

        @pl.loop(0, rows // 16)
        def _(n):
            r = pl.ds(pl.multiple_of(n * 16, 16), 16)
            wide = acc[r, :]
            scale = lax.rsqrt(jnp.sum(wide * wide, axis=-1, keepdims=True) * (1.0 / rank) + EPS)
            lat[pl.ds(pl.multiple_of(j * rows + n * 16, 16), 16), :] = (wide * scale * kvg_ref[...]).astype(
                jnp.bfloat16
            )

        if DO_L:
            for d in range(n_x):
                q = wrap(x + d, n_x)
                own = jnp.logical_and(has_self, 2 * t + j == z) if d == 0 else False
                src, dst = own_piece(j, q), place_of(z, q)

                def remote(src=src, dst=dst, q=q):
                    send(src, dst, dev(q, home, 2 * t + j), lsend.at[0, j], dir_sem.at[z // 2])

                if d == 0:
                    pl.when(own)(
                        lambda src=src, dst=dst: pltpu.make_async_copy(src, dst, dir_sem.at[z // 2]).start()
                    )
                    pl.when(jnp.logical_not(own))(remote)
                else:
                    remote()

    near = [0] + [v for k in range(2, steps, 2) for v in (k, -k)] + [steps]
    odd = [v for k in range(1, steps, 2) for v in (k, -k)]
    same = home == c
    sources = [wrap(z + jnp.where(same, a, b), n_sp) for a, b in zip(near, odd)]
    n_src = len(sources)

    def direct(n):
        s = sources[n]
        ref = place_of(s, x)
        arrived(ref, dir_sem.at[s // 2])
        send(ref, ref, right, lsend.at[1, 0], lx_sem.at[0, n])
        send(ref, ref, left, lsend.at[1, 1], lx_sem.at[1, n])

    def beside(n):
        s = sources[n]
        from_left, from_right = place_of(s, wrap(x - 1, n_x)), place_of(s, wrap(x + 1, n_x))
        arrived(from_left, lx_sem.at[0, n])
        if n % 2 == 0:
            send(from_left, from_left, right, lsend.at[2, 0], lx_sem.at[2, n])
        arrived(from_right, lx_sem.at[1, n])
        if n % 2 == 1:
            send(from_right, from_right, left, lsend.at[2, 0], lx_sem.at[2, n])

    def block(s):
        return latall.at[pl.ds(pl.multiple_of(s * rows, rows), rows)]

    def far(n):
        s = sources[n]
        arrived(place_of(s, wrap(x + 2, n_x)), lx_sem.at[2, n])
        send(block(s), block(s), partner, lsend.at[2, 1], lp_sem.at[s])

    def up_project(s):
        r = pl.ds(pl.multiple_of(s * rows, rows), rows)
        both = jnp.dot(latall[r, :], wup[...], preferred_element_type=jnp.float32).astype(jnp.bfloat16)
        keys_ref[r, :] = both[:, :heads]
        values_ref[r, :] = both[:, heads:]

    loads[2].wait()
    loads[3].wait()
    if DO_L:
        for n in range(n_src + 2):
            if n < n_src:
                direct(n)
            if 1 <= n <= n_src:
                beside(n - 1)
            if 2 <= n:
                far(n - 2)
        other = [wrap(z + jnp.where(same, b, a), n_sp) for a, b in zip(near, odd)]
        for n in range(n_src):
            arrived(block(other[n]), lp_sem.at[other[n]])
    if DO_C:
        @pl.loop(0, n_sp)
        def _(s):
            up_project(s)

    for s in range(n_sp):
        mine = jnp.logical_and(lax.rem(s // 2, n_x) == x, s % 2 == c)

        @pl.when(jnp.logical_not(mine))
        def _():
            arrived(rope_block(s), rsem.at[s])

    for j in range(2):
        own = jnp.logical_and(has_self, jnp.logical_and(2 * t + j == z, x == column))

        @pl.when(jnp.logical_not(own))
        def _():
            arrived(ropeown.at[j], rsend.at[0, j])

    for g in range(n_sp // 2 // n_x):
        for n in range(len(peers)):
            arrived(ropeown.at[0], rsend.at[1 + g, n])
    if DO_W:
        for sign in (1, -1):
            for _ in range(1):
                f_rows, q_rows = limit["f", sign] * FULL, limit["q", sign] * (half - FULL)
                arrived(wfull.at[pl.ds(0, f_rows)], wsend.at[int(sign < 0)])
                arrived(wfull.at[pl.ds(0, q_rows), pl.ds(0, quarter)], wsend.at[2 + int(sign < 0)])
        q_rows = (2 * steps - 1) * (half - FULL)
        for row in (4, 5, 6):
            arrived(wfull.at[pl.ds(0, q_rows), pl.ds(0, quarter)], wsend.at[row])
        arrived(wfull.at[pl.ds(0, (2 * steps - 1) * half)], wsend.at[7])
    if DO_L:
        for j in range(2):
            own = jnp.logical_and(has_self, 2 * t + j == z)
            pl.when(own)(lambda: arrived(lat.at[pl.ds(0, rows - piece)], lsend.at[0, j]))
            pl.when(jnp.logical_not(own))(lambda: arrived(lat.at[pl.ds(0, rows)], lsend.at[0, j]))
        for a, b in ((1, 0), (1, 1), (2, 0)):
            arrived(latall.at[pl.ds(0, n_src * piece)], lsend.at[a, b])
        arrived(latall.at[pl.ds(0, n_src * rows)], lsend.at[2, 1])


def attend(
    keys_ref, values_ref, rope_ref, qn_ref, qr_ref, keys_out, values_out, rope_out, read_ref, sem
):
    outs = [
        pltpu.make_async_copy(keys_ref, keys_out, sem.at[0]),
        pltpu.make_async_copy(values_ref, values_out, sem.at[1]),
        pltpu.make_async_copy(rope_ref, rope_out, sem.at[2]),
    ]
    for out in outs:
        out.start()
    heads = keys_ref.shape[1] // HEAD
    rot = qr_ref.shape[1] // heads
    pad = 8

    def by_head(ref, size):
        wide = jnp.broadcast_to(ref[...].astype(jnp.float32), (pad, ref.shape[1]))
        row = lax.broadcasted_iota(jnp.int32, wide.shape, 0)
        col = lax.broadcasted_iota(jnp.int32, wide.shape, 1)
        return jnp.where(col // size == row, wide, 0.0)

    nope = by_head(qn_ref, HEAD).astype(jnp.bfloat16)
    scores = lax.dot_general(
        nope, keys_ref[...], (((1,), (1,)), ((), ())), preferred_element_type=jnp.float32
    )
    spread = by_head(qr_ref, rot)
    rotary = spread[:, :rot]
    for h in range(1, heads):
        rotary = rotary + spread[:, h * rot:(h + 1) * rot]
    scores = scores + jnp.dot(
        rotary.astype(jnp.bfloat16), rope_ref[...], preferred_element_type=jnp.float32
    )
    scores = scores / jnp.sqrt(jnp.float32(HEAD + ROPE))
    expo = jnp.exp(scores - jnp.max(scores, axis=-1, keepdims=True))
    weights = (expo / jnp.sum(expo, axis=-1, keepdims=True)).astype(jnp.bfloat16)
    read = jnp.dot(weights, values_ref[...], preferred_element_type=jnp.float32)
    row = lax.broadcasted_iota(jnp.int32, read.shape, 0)
    col = lax.broadcasted_iota(jnp.int32, read.shape, 1)
    read_ref[...] = jnp.sum(
        jnp.where(col // HEAD == row, read, 0.0), axis=0, keepdims=True
    ).astype(jnp.bfloat16)
    for out in outs:
        out.wait()


def local(
    n_sp, n_tp,
    tokens, offsets, in_gain, w_latent, w_rope_key, kv_gain, w_up_key, w_up_value, q_nope, q_rope
):
    prompts, rows, width = tokens.shape
    depth, rank = w_latent.shape
    heads = w_up_key.shape[1]
    length = n_sp * rows
    steps = n_sp // 2
    any_space = pl.BlockSpec(memory_space=pl.ANY)
    vmem = pl.BlockSpec(memory_space=pltpu.VMEM)
    smem = pl.BlockSpec(memory_space=pltpu.SMEM)
    dma = pltpu.SemaphoreType.DMA
    keys, values, rope = pl.pallas_call(
        functools.partial(exchange, n_sp, n_tp),
        out_shape=(
            jax.ShapeDtypeStruct((length, heads), jnp.bfloat16),
            jax.ShapeDtypeStruct((length, heads), jnp.bfloat16),
            jax.ShapeDtypeStruct((ROPE, length), jnp.bfloat16),
        ),
        in_specs=[any_space, smem, vmem, any_space, vmem, vmem, any_space, any_space],
        out_specs=(vmem, vmem, vmem),
        scratch_shapes=[
            pltpu.VMEM((prompts * rows, width), jnp.bfloat16),
            pltpu.VMEM((width, rank), jnp.bfloat16),
            pltpu.VMEM((rank, 2 * heads), jnp.bfloat16),
            pltpu.VMEM((prompts * rows, rank), jnp.bfloat16),
            pltpu.VMEM((rows, rank), jnp.float32),
            pltpu.VMEM((length, rank), jnp.bfloat16),
            pltpu.VMEM((prompts, ROPE, rows), jnp.bfloat16),
            dma((4,)),
            dma((4, steps)),
            dma((3, 2 * steps - 1)),
            dma((2 * steps - 1,)),
            dma((8,)),
            dma((steps,)),
            dma((3, steps)),
            dma((n_sp,)),
            dma((3, 2)),
            dma((n_sp,)),
            dma((1 + n_sp // n_tp, n_tp - 1)),
        ],
        compiler_params=pltpu.CompilerParams(
            collective_id=0, has_side_effects=True, vmem_limit_bytes=48 * 1024 * 1024
        ),
        name="exchange",
    )(
        tokens.reshape(prompts * rows, width), offsets, in_gain.reshape(1, width), w_latent,
        w_rope_key.T, kv_gain.reshape(1, rank), w_up_key, w_up_value,
    )
    return pl.pallas_call(
        attend,
        out_shape=(
            jax.ShapeDtypeStruct((length, heads), jnp.bfloat16),
            jax.ShapeDtypeStruct((length, heads), jnp.bfloat16),
            jax.ShapeDtypeStruct((ROPE, length), jnp.bfloat16),
            jax.ShapeDtypeStruct((1, heads), jnp.bfloat16),
        ),
        in_specs=[vmem] * 5,
        out_specs=(any_space, any_space, any_space, vmem),
        scratch_shapes=[dma((3,))],
        compiler_params=pltpu.CompilerParams(vmem_limit_bytes=24 * 1024 * 1024),
        name="attend",
    )(keys, values, rope, q_nope, q_rope)


def solution(mesh):
    n_sp, n_tp = mesh.shape["sp"], mesh.shape["tp"]

    def body(*args):
        keys, values, rope, read = local(n_sp, n_tp, *args)
        return keys[None], values[None], rope[None], read

    in_specs = (
        P(("grp", "tp"), "sp", None),
        P(("grp", "tp")),
        P(),
        P("sp", None),
        P(),
        P(),
        P(None, "tp"),
        P(None, "tp"),
        P(("grp", "sp"), "tp"),
        P(("grp", "sp"), "tp"),
    )
    out_specs = (
        P(("grp", "sp"), None, "tp"),
        P(("grp", "sp"), None, "tp"),
        P(("grp", "sp"), None, None),
        P(("grp", "sp"), "tp"),
    )
    return jax.shard_map(body, mesh=mesh, in_specs=in_specs, out_specs=out_specs, check_vma=False)
```

```python
import functools

import jax
import jax.numpy as jnp
from jax import lax
from jax.experimental import pallas as pl
from jax.experimental.pallas import tpu as pltpu
from jax.sharding import PartitionSpec as P

HEAD = 64
ROPE = 32
EPS = 1e-06
MESH = pl.DeviceIdType.MESH
FULL = 48

HALVES = 2


def exchange(
    n_sp, n_tp, tok_hbm, off_ref, gain_hbm, wl_hbm, wrope_hbm, kvg_hbm, wk_hbm, wv_hbm,
    keys_ref, values_ref, rope_ref,
    norm, wfull, wup, lat, acc, latall, ropeown, stage, gain_ref, wrope_ref, kvg_ref,
    local_sem, wz_sem, wx_sem, wp_sem, wsend, a_sem, dir_sem, lx_sem, lp_sem, lsend, rsem, rsend,
):
    z = lax.axis_index("sp")
    t = lax.axis_index("tp")
    n_x = n_tp // 2
    x, c = t // 2, lax.rem(t, 2)
    rows = norm.shape[0] // 2
    width = norm.shape[1]
    rank = lat.shape[1]
    depth = width // n_sp
    half = depth // 2
    quarter = rank // n_x
    piece = rows // n_x
    heads = keys_ref.shape[1]

    def wrap(v, n):
        return lax.rem(v + 2 * n, n)

    def dev(xx, cc, zz):
        return {"sp": zz, "tp": 2 * xx + cc}

    z_next, z_prev = wrap(z + 1, n_sp), wrap(z - 1, n_sp)
    right = dev(wrap(x + 1, n_x), c, z)
    left = dev(wrap(x - 1, n_x), c, z)
    up = dev(x, c, z_next)
    down = dev(x, c, z_prev)
    partner = dev(x, 1 - c, z)
    home = lax.rem(z, 2)
    src_x, src_c = z // 4, lax.rem(z // 2, 2)
    has_self = jnp.logical_and(src_c == c, c == home)

    loads = [
        pltpu.make_async_copy(wl_hbm, wfull.at[pl.ds(z * depth, depth)], local_sem.at[0]),
        pltpu.make_async_copy(tok_hbm, norm, local_sem.at[1]),
        pltpu.make_async_copy(wk_hbm, wup.at[:, pl.ds(0, heads)], local_sem.at[2]),
        pltpu.make_async_copy(wv_hbm, wup.at[:, pl.ds(heads, heads)], local_sem.at[3]),
        pltpu.make_async_copy(gain_hbm, gain_ref, local_sem.at[4]),
        pltpu.make_async_copy(wrope_hbm, wrope_ref, local_sem.at[5]),
        pltpu.make_async_copy(kvg_hbm, kvg_ref, local_sem.at[6]),
    ]
    for load in loads:
        load.start()

    barrier = pltpu.get_barrier_semaphore()

    def greet(device):
        pl.semaphore_signal(barrier, inc=1, device_id=device, device_id_type=MESH)

    column = lax.rem(z // 2, n_x)
    rope_self = jnp.logical_and(jnp.logical_and(x == src_x, c == src_c), jnp.logical_and(x == column, c == home))
    around = (right, left, up, down, partner)
    for device in around:
        greet(device)
    pl.semaphore_wait(barrier, len(around))

    def send(src, dst, device, send_sem, recv_sem):
        pltpu.make_async_remote_copy(
            src_ref=src, dst_ref=dst, send_sem=send_sem, recv_sem=recv_sem,
            device_id=device, device_id_type=MESH,
        ).start()

    def arrived(dst, recv_sem):
        pltpu.make_async_copy(dst, dst, recv_sem).wait()

    def w_full(s):
        return wfull.at[pl.ds(s * depth + c * half, FULL)]

    def w_part(s, xx):
        return wfull.at[
            pl.ds(s * depth + c * half + FULL, half - FULL), pl.ds(pl.multiple_of(xx * quarter, quarter), quarter)
        ]

    def w_half(s, cc):
        return wfull.at[pl.ds(s * depth + cc * half, half)]

    steps = n_sp // 2
    limit = {("f", 1): steps, ("f", -1): steps - 1, ("q", 1): steps - 1, ("q", -1): steps}

    def z_send(kind, sign, k):
        s = wrap(z - sign * k, n_sp)
        ref = w_full(s) if kind == "f" else w_part(s, x)
        row = ("f", "q").index(kind) * 2 + (sign < 0)
        send(ref, ref, up if sign > 0 else down, wsend.at[row], wz_sem.at[row, k])

    def z_arrive(kind, sign, k):
        s = wrap(z - sign * k, n_sp)
        ref = w_full(s) if kind == "f" else w_part(s, x)
        row = ("f", "q").index(kind) * 2 + (sign < 0)
        arrived(ref, wz_sem.at[row, k - 1])
        if k < limit[kind, sign]:
            z_send(kind, sign, k)
        if kind == "q":
            col = k - 1 if sign > 0 else steps + k - 2
            send(ref, ref, right, wsend.at[4], wx_sem.at[0, col])
            send(ref, ref, left, wsend.at[5], wx_sem.at[1, col])

    def x_arrive(sign, k):
        s = wrap(z - sign * k, n_sp)
        col = k - 1 if sign > 0 else steps + k - 2
        from_left, from_right = w_part(s, wrap(x - 1, n_x)), w_part(s, wrap(x + 1, n_x))
        arrived(from_left, wx_sem.at[0, col])
        if sign > 0:
            send(from_left, from_left, right, wsend.at[6], wx_sem.at[2, col])
        arrived(from_right, wx_sem.at[1, col])
        if sign < 0:
            send(from_right, from_right, left, wsend.at[6], wx_sem.at[2, col])

    def far_arrive(sign, k):
        s = wrap(z - sign * k, n_sp)
        col = k - 1 if sign > 0 else steps + k - 2
        far = w_part(s, wrap(x + 2, n_x))
        arrived(far, wx_sem.at[2, col])
        ref = w_half(s, c)
        send(ref, ref, partner, wsend.at[7], wp_sem.at[col])

    loads[0].wait()
    if True:
        for kind in ("f", "q"):
            for sign in (1, -1):
                z_send(kind, sign, 0)

    loads[1].wait()
    loads[4].wait()
    loads[5].wait()
    loads[6].wait()

    def normalise(part, parts):
        @pl.loop(part * 2 * rows // 16 // parts, (part + 1) * 2 * rows // 16 // parts)
        def _(n):
            r = pl.ds(pl.multiple_of(n * 16, 16), 16)
            wide = norm[r, :].astype(jnp.float32)
            scale = lax.rsqrt(jnp.sum(wide * wide, axis=-1, keepdims=True) * (1.0 / width) + EPS)
            norm[r, :] = (wide * scale * gain_ref[...]).astype(jnp.bfloat16)

    def partial(s, first=False):
        @pl.loop(0, n_x)
        def _(n):
            cols = pl.ds(pl.multiple_of(n * quarter, quarter), quarter)
            term = jnp.dot(
                norm[:, pl.ds(pl.multiple_of(s * depth, depth), depth)],
                wfull[pl.ds(pl.multiple_of(s * depth, depth), depth), cols],
                preferred_element_type=jnp.float32,
            )
            acc[:, cols] = term if first else acc[:, cols] + term

    def finish(sign, k):
        s = wrap(z - sign * k, n_sp)
        col = k - 1 if sign > 0 else steps + k - 2
        arrived(w_half(s, 1 - c), wp_sem.at[col])
        partial(s)

    def rotary():
        raw = lax.dot_general(
            wrope_ref[...], norm[...], (((1,), (1,)), ((), ())), preferred_element_type=jnp.float32
        )
        index = lax.broadcasted_iota(jnp.int32, (ROPE // 2, rows), 0).astype(jnp.float32) * 2.0
        inverse = jnp.exp(index * (-jnp.log(jnp.float32(10000.0)) / ROPE))
        place = lax.broadcasted_iota(jnp.int32, (ROPE // 2, rows), 1)
        for j in range(2):
            angle = (off_ref[j] + z * rows + place).astype(jnp.float32) * inverse
            cosine, sine = jnp.cos(angle), jnp.sin(angle)
            first = raw[: ROPE // 2, j * rows:(j + 1) * rows]
            second = raw[ROPE // 2:, j * rows:(j + 1) * rows]
            ropeown[j] = jnp.concatenate(
                [first * cosine - second * sine, second * cosine + first * sine], axis=0
            ).astype(jnp.bfloat16)

    normalise(0, 4)
    if True:
        for k in range(1, steps + 1):
            for sign in (1, -1):
                for kind in ("q", "f"):
                    if k <= limit[kind, sign]:
                        z_arrive(kind, sign, k)
            if k < 4:
                normalise(k, 4)
            for sign in (1, -1):
                if 1 <= k - 1 <= limit["q", sign]:
                    x_arrive(sign, k - 1)
            for sign in (1, -1):
                if 1 <= k - 2 <= limit["q", sign]:
                    far_arrive(sign, k - 2)
            if k == 3:
                partial(z, True)
            if k == 4:
                rotary()
            for sign in (1, -1):
                if 1 <= k - 3:
                    finish(sign, k - 3)
        x_arrive(-1, steps)
        for sign in (1, -1):
            far_arrive(sign, steps - 1)
        for sign in (1, -1):
            finish(sign, steps - 2)
        far_arrive(-1, steps)
        for sign in (1, -1):
            finish(sign, steps - 1)
        finish(-1, steps)

    for j in range(2):
        own = jnp.logical_and(rope_self, 2 * t + j == z)
        dst = rope_ref.at[:, pl.ds(pl.multiple_of(z * rows, rows), rows)]

        @pl.when(own)
        def _():
            pltpu.make_async_copy(ropeown.at[j], dst, rsem.at[z]).start()

        @pl.when(jnp.logical_not(own))
        def _():
            send(ropeown.at[j], dst, dev(column, home, 2 * t + j), rsend.at[0, j], rsem.at[z])

    small = piece // HALVES

    def own_piece(j, q, h):
        return lat.at[pl.ds(pl.multiple_of(j * rows + q * piece + h * small, small), small)]

    def staged(xx, j, h):
        return stage.at[xx, j, pl.ds(h * small, small)]

    def place_of(s, q, h):
        return latall.at[pl.ds(pl.multiple_of(s * rows + q * piece + h * small, small), small)]

    for j in range(2):
        @pl.loop(j * rows // 16, (j + 1) * rows // 16)
        def _(n):
            r = pl.ds(pl.multiple_of(n * 16, 16), 16)
            wide = acc[r, :]
            scale = lax.rsqrt(jnp.sum(wide * wide, axis=-1, keepdims=True) * (1.0 / rank) + EPS)
            lat[r, :] = (wide * scale * kvg_ref[...]).astype(jnp.bfloat16)

        stage[x, j] = lat[pl.ds(pl.multiple_of(j * rows + x * piece, piece), piece), :]
        for h in range(HALVES):
            for d in (2, 1, -1):
                q = wrap(x + d, n_x)
                send(own_piece(j, q, h), staged(x, j, h), dev(q, c, z), lsend.at[0, j], a_sem.at[x, j, h])

    origin = lax.rem(z - 2 * c + n_sp, n_sp) // 4
    for d in (0, 1, -1, 2):
        xx = wrap(origin + d, n_x)
        for j in range(2):
            goal = 4 * xx + 2 * c + j
            own = jnp.logical_and(has_self, goal == z)
            for h in range(HALVES):
                @pl.when(xx != x)
                def _():
                    arrived(staged(xx, j, h), a_sem.at[xx, j, h])

                src, dst, sem = staged(xx, j, h), place_of(z, x, h), dir_sem.at[z // 2, h]

                @pl.when(own)
                def _():
                    pltpu.make_async_copy(src, dst, sem).start()

                @pl.when(jnp.logical_not(own))
                def _():
                    send(src, dst, dev(x, home, goal), lsend.at[3, 0], sem)

    near = [0] + [v for k in range(2, steps, 2) for v in (k, -k)] + [steps]
    odd = [v for k in range(1, steps, 2) for v in (k, -k)]
    same = home == c
    sources = [wrap(z + jnp.where(same, a, b), n_sp) for a, b in zip(near, odd)]
    other = [wrap(z + jnp.where(same, b, a), n_sp) for a, b in zip(near, odd)]
    n_src = len(sources)

    def direct(n, h):
        s = sources[n]
        ref = place_of(s, x, h)
        arrived(ref, dir_sem.at[s // 2, h])
        send(ref, ref, right, lsend.at[1, 0], lx_sem.at[0, n, h])
        send(ref, ref, left, lsend.at[1, 1], lx_sem.at[1, n, h])

    def beside(n, h):
        s = sources[n]
        from_left, from_right = place_of(s, wrap(x - 1, n_x), h), place_of(s, wrap(x + 1, n_x), h)
        arrived(from_left, lx_sem.at[0, n, h])
        if (n + h) % 2 == 0:
            send(from_left, from_left, right, lsend.at[2, 0], lx_sem.at[2, n, h])
        arrived(from_right, lx_sem.at[1, n, h])
        if (n + h) % 2 == 1:
            send(from_right, from_right, left, lsend.at[2, 0], lx_sem.at[2, n, h])

    def block(s):
        return latall.at[pl.ds(pl.multiple_of(s * rows, rows), rows)]

    def far(n, h):
        s = sources[n]
        arrived(place_of(s, wrap(x + 2, n_x), h), lx_sem.at[2, n, h])
        if h == HALVES - 1:
            send(block(s), block(s), partner, lsend.at[2, 1], lp_sem.at[s])

    def up_project(s):
        r = pl.ds(pl.multiple_of(s * rows, rows), rows)
        both = jnp.dot(latall[r, :], wup[...], preferred_element_type=jnp.float32).astype(jnp.bfloat16)
        keys_ref[r, :] = both[:, :heads]
        values_ref[r, :] = both[:, heads:]

    def rope_block(s):
        return rope_ref.at[:, pl.ds(pl.multiple_of(s * rows, rows), rows)]

    peers = [(dx, dc) for dx in range(n_x) for dc in range(2) if dx or dc]
    def rope_onward():
        for g in range(n_sp // 2 // n_x):
            s = 2 * (x + n_x * g) + c
            arrived(rope_block(s), rsem.at[s])
            for n, (dx, dc) in enumerate(peers):
                send(
                    rope_block(s), rope_block(s), dev(wrap(x + dx, n_x), lax.rem(c + dc, 2), z),
                    rsend.at[1 + g, n], rsem.at[s],
                )

    loads[2].wait()
    loads[3].wait()
    order = [(n, h) for n in range(n_src) for h in range(HALVES)]
    for i in range(len(order) + 2):
        if i < len(order):
            direct(*order[i])
        if 1 <= i <= len(order):
            beside(*order[i - 1])
        if i == 6:
            rope_onward()
        if 2 <= i:
            far(*order[i - 2])
            n, h = order[i - 2]
            if h == HALVES - 1:
                up_project(sources[n])
            elif n >= 1:
                arrived(block(other[n - 1]), lp_sem.at[other[n - 1]])
                up_project(other[n - 1])
    arrived(block(other[n_src - 1]), lp_sem.at[other[n_src - 1]])
    up_project(other[n_src - 1])

    for s in range(n_sp):
        mine = jnp.logical_and(lax.rem(s // 2, n_x) == x, s % 2 == c)

        @pl.when(jnp.logical_not(mine))
        def _():
            arrived(rope_block(s), rsem.at[s])

    for j in range(2):
        own = jnp.logical_and(rope_self, 2 * t + j == z)

        @pl.when(jnp.logical_not(own))
        def _():
            arrived(ropeown.at[j], rsend.at[0, j])

    for g in range(n_sp // 2 // n_x):
        for n in range(len(peers)):
            arrived(ropeown.at[0], rsend.at[1 + g, n])
    if True:
        for sign in (1, -1):
            for _ in range(1):
                f_rows, q_rows = limit["f", sign] * FULL, limit["q", sign] * (half - FULL)
                arrived(wfull.at[pl.ds(0, f_rows)], wsend.at[int(sign < 0)])
                arrived(wfull.at[pl.ds(0, q_rows), pl.ds(0, quarter)], wsend.at[2 + int(sign < 0)])
        q_rows = (2 * steps - 1) * (half - FULL)
        for row in (4, 5, 6):
            arrived(wfull.at[pl.ds(0, q_rows), pl.ds(0, quarter)], wsend.at[row])
        arrived(wfull.at[pl.ds(0, (2 * steps - 1) * half)], wsend.at[7])
    if True:
        for j in range(2):
            arrived(lat.at[pl.ds(0, rows - piece)], lsend.at[0, j])
        pl.when(has_self)(lambda: arrived(lat.at[pl.ds(0, 2 * rows - piece)], lsend.at[3, 0]))
        pl.when(jnp.logical_not(has_self))(lambda: arrived(lat, lsend.at[3, 0]))
        for a, b in ((1, 0), (1, 1), (2, 0)):
            arrived(latall.at[pl.ds(0, n_src * piece)], lsend.at[a, b])
        arrived(latall.at[pl.ds(0, n_src * rows)], lsend.at[2, 1])


def in_hbm(value):
    return pltpu.with_memory_space_constraint(value, pltpu.HBM)


def attend(
    keys_ref, values_ref, rope_ref, qn_ref, qr_ref, keys_out, values_out, rope_out, read_ref, sem
):
    outs = [
        pltpu.make_async_copy(keys_ref, keys_out, sem.at[0]),
        pltpu.make_async_copy(values_ref, values_out, sem.at[1]),
        pltpu.make_async_copy(rope_ref, rope_out, sem.at[2]),
    ]
    for out in outs:
        out.start()
    heads = keys_ref.shape[1] // HEAD
    rot = qr_ref.shape[1] // heads
    pad = 8

    def by_head(ref, size):
        wide = jnp.broadcast_to(ref[...].astype(jnp.float32), (pad, ref.shape[1]))
        row = lax.broadcasted_iota(jnp.int32, wide.shape, 0)
        col = lax.broadcasted_iota(jnp.int32, wide.shape, 1)
        return jnp.where(col // size == row, wide, 0.0)

    nope = by_head(qn_ref, HEAD).astype(jnp.bfloat16)
    scores = lax.dot_general(
        nope, keys_ref[...], (((1,), (1,)), ((), ())), preferred_element_type=jnp.float32
    )
    spread = by_head(qr_ref, rot)
    rotary = spread[:, :rot]
    for h in range(1, heads):
        rotary = rotary + spread[:, h * rot:(h + 1) * rot]
    scores = scores + jnp.dot(
        rotary.astype(jnp.bfloat16), rope_ref[...], preferred_element_type=jnp.float32
    )
    scores = scores / jnp.sqrt(jnp.float32(HEAD + ROPE))
    expo = jnp.exp(scores - jnp.max(scores, axis=-1, keepdims=True))
    weights = (expo / jnp.sum(expo, axis=-1, keepdims=True)).astype(jnp.bfloat16)
    read = jnp.dot(weights, values_ref[...], preferred_element_type=jnp.float32)
    row = lax.broadcasted_iota(jnp.int32, read.shape, 0)
    col = lax.broadcasted_iota(jnp.int32, read.shape, 1)
    read_ref[...] = jnp.sum(
        jnp.where(col // HEAD == row, read, 0.0), axis=0, keepdims=True
    ).astype(jnp.bfloat16)
    for out in outs:
        out.wait()


def local(
    n_sp, n_tp,
    tokens, offsets, in_gain, w_latent, w_rope_key, kv_gain, w_up_key, w_up_value, q_nope, q_rope
):
    prompts, rows, width = tokens.shape
    depth, rank = w_latent.shape
    heads = w_up_key.shape[1]
    length = n_sp * rows
    steps = n_sp // 2
    any_space = pl.BlockSpec(memory_space=pl.ANY)
    hbm = pl.BlockSpec(memory_space=pltpu.HBM)
    vmem = pl.BlockSpec(memory_space=pltpu.VMEM)
    smem = pl.BlockSpec(memory_space=pltpu.SMEM)
    dma = pltpu.SemaphoreType.DMA
    keys, values, rope = pl.pallas_call(
        functools.partial(exchange, n_sp, n_tp),
        out_shape=(
            jax.ShapeDtypeStruct((length, heads), jnp.bfloat16),
            jax.ShapeDtypeStruct((length, heads), jnp.bfloat16),
            jax.ShapeDtypeStruct((ROPE, length), jnp.bfloat16),
        ),
        in_specs=[hbm, smem, hbm, hbm, hbm, hbm, hbm, hbm],
        out_specs=(vmem, vmem, vmem),
        scratch_shapes=[
            pltpu.VMEM((prompts * rows, width), jnp.bfloat16),
            pltpu.VMEM((width, rank), jnp.bfloat16),
            pltpu.VMEM((rank, 2 * heads), jnp.bfloat16),
            pltpu.VMEM((prompts * rows, rank), jnp.bfloat16),
            pltpu.VMEM((prompts * rows, rank), jnp.float32),
            pltpu.VMEM((length, rank), jnp.bfloat16),
            pltpu.VMEM((prompts, ROPE, rows), jnp.bfloat16),
            pltpu.VMEM((n_tp // 2, prompts, rows * 2 // n_tp, rank), jnp.bfloat16),
            pltpu.VMEM((1, width), jnp.float32),
            pltpu.VMEM((ROPE, width), jnp.bfloat16),
            pltpu.VMEM((1, rank), jnp.float32),
            dma((7,)),
            dma((4, steps)),
            dma((3, 2 * steps - 1)),
            dma((2 * steps - 1,)),
            dma((8,)),
            dma((n_tp // 2, prompts, HALVES)),
            dma((steps, HALVES)),
            dma((3, steps, HALVES)),
            dma((n_sp,)),
            dma((4, 2)),
            dma((n_sp,)),
            dma((1 + n_sp // n_tp, n_tp - 1)),
        ],
        compiler_params=pltpu.CompilerParams(
            collective_id=0, has_side_effects=True, vmem_limit_bytes=40 * 1024 * 1024
        ),
        name="exchange",
    )(
        *map(
            in_hbm,
            (tokens.reshape(prompts * rows, width),),
        ),
        offsets,
        *map(
            in_hbm,
            (
                in_gain.reshape(1, width), w_latent, w_rope_key.T, kv_gain.reshape(1, rank),
                w_up_key, w_up_value,
            ),
        ),
    )
    return pl.pallas_call(
        attend,
        out_shape=(
            jax.ShapeDtypeStruct((length, heads), jnp.bfloat16),
            jax.ShapeDtypeStruct((length, heads), jnp.bfloat16),
            jax.ShapeDtypeStruct((ROPE, length), jnp.bfloat16),
            jax.ShapeDtypeStruct((1, heads), jnp.bfloat16),
        ),
        in_specs=[vmem] * 5,
        out_specs=(any_space, any_space, any_space, vmem),
        scratch_shapes=[dma((3,))],
        compiler_params=pltpu.CompilerParams(vmem_limit_bytes=24 * 1024 * 1024),
        name="attend",
    )(keys, values, rope, q_nope, q_rope)


def solution(mesh):
    n_sp, n_tp = mesh.shape["sp"], mesh.shape["tp"]

    def body(*args):
        keys, values, rope, read = local(n_sp, n_tp, *args)
        return keys[None], values[None], rope[None], read

    in_specs = (
        P(("grp", "tp"), "sp", None),
        P(("grp", "tp")),
        P(),
        P("sp", None),
        P(),
        P(),
        P(None, "tp"),
        P(None, "tp"),
        P(("grp", "sp"), "tp"),
        P(("grp", "sp"), "tp"),
    )
    out_specs = (
        P(("grp", "sp"), None, "tp"),
        P(("grp", "sp"), None, "tp"),
        P(("grp", "sp"), None, None),
        P(("grp", "sp"), "tp"),
    )
    return jax.shard_map(body, mesh=mesh, in_specs=in_specs, out_specs=out_specs, check_vma=False)
```

```python
import functools

import jax
import jax.numpy as jnp
from jax import lax
from jax.experimental import pallas as pl
from jax.experimental.pallas import tpu as pltpu
from jax.sharding import PartitionSpec as P

HEAD = 64
ROPE = 32
EPS = 1e-06
MESH = pl.DeviceIdType.MESH
WX = 5
FULL = 96

LAGS = (1, 3, 4)
HALVES = 2
PARTS = (2, 3)


def exchange(
    n_sp, n_tp, tok_hbm, off_ref, gain_hbm, wl_hbm, wrope_hbm, kvg_hbm, wk_hbm, wv_hbm,
    keys_ref, values_ref, rope_ref,
    norm, wfull, wup, lat, acc, latall, ropeown, stage, gain_ref, wrope_ref, kvg_ref,
    local_sem, wz_sem, wx_sem, wp_sem, wsend, a_sem, dir_sem, lx_sem, lp_sem, lsend, rsem, rsend,
):
    z = lax.axis_index("sp")
    t = lax.axis_index("tp")
    n_x = n_tp // 2
    x, c = t // 2, lax.rem(t, 2)
    rows = norm.shape[0] // 2
    width = norm.shape[1]
    rank = lat.shape[1]
    depth = width // n_sp
    quarter = rank // n_x
    piece = rows // n_x
    heads = keys_ref.shape[1]

    def wrap(v, n):
        return lax.rem(v + 2 * n, n)

    def dev(xx, cc, zz):
        return {"sp": zz, "tp": 2 * xx + cc}

    z_next, z_prev = wrap(z + 1, n_sp), wrap(z - 1, n_sp)
    right = dev(wrap(x + 1, n_x), c, z)
    left = dev(wrap(x - 1, n_x), c, z)
    up = dev(x, c, z_next)
    down = dev(x, c, z_prev)
    partner = dev(x, 1 - c, z)
    home = lax.rem(z, 2)
    src_x, src_c = z // 4, lax.rem(z // 2, 2)
    has_self = jnp.logical_and(src_c == c, c == home)

    loads = [
        pltpu.make_async_copy(wl_hbm, wfull.at[pl.ds(z * depth, depth)], local_sem.at[0]),
        pltpu.make_async_copy(tok_hbm, norm, local_sem.at[1]),
        pltpu.make_async_copy(wk_hbm, wup.at[:, pl.ds(0, heads)], local_sem.at[2]),
        pltpu.make_async_copy(wv_hbm, wup.at[:, pl.ds(heads, heads)], local_sem.at[3]),
        pltpu.make_async_copy(gain_hbm, gain_ref, local_sem.at[4]),
        pltpu.make_async_copy(wrope_hbm, wrope_ref, local_sem.at[5]),
        pltpu.make_async_copy(kvg_hbm, kvg_ref, local_sem.at[6]),
    ]
    for load in loads:
        load.start()

    barrier = pltpu.get_barrier_semaphore()

    def greet(device):
        pl.semaphore_signal(barrier, inc=1, device_id=device, device_id_type=MESH)

    column = lax.rem(z // 2, n_x)
    rope_self = jnp.logical_and(jnp.logical_and(x == src_x, c == src_c), jnp.logical_and(x == column, c == home))
    around = (right, left, up, down, partner)
    for device in around:
        greet(device)
    pl.semaphore_wait(barrier, len(around))

    def send(src, dst, device, send_sem, recv_sem):
        pltpu.make_async_remote_copy(
            src_ref=src, dst_ref=dst, send_sem=send_sem, recv_sem=recv_sem,
            device_id=device, device_id_type=MESH,
        ).start()

    def arrived(dst, recv_sem):
        pltpu.make_async_copy(dst, dst, recv_sem).wait()

    sign = 1 - 2 * c
    onward = dev(x, c, wrap(z + sign, n_sp))
    ahead, behind = dev(wrap(x + sign, n_x), c, z), dev(wrap(x - sign, n_x), c, z)
    q_part, f_part = (depth - FULL) // PARTS[0], FULL // PARTS[1]
    parts = [("q", i) for i in range(PARTS[0])] + [("f", i) for i in range(PARTS[1])]

    def w_part(s, xx):
        return wfull.at[
            pl.ds(pl.multiple_of(s * depth + FULL, 32), depth - FULL),
            pl.ds(pl.multiple_of(xx * quarter, quarter), quarter),
        ]

    def w_message(s, kind, i):
        if kind == "f":
            return wfull.at[pl.ds(pl.multiple_of(s * depth + i * f_part, f_part), f_part)]
        return wfull.at[
            pl.ds(pl.multiple_of(s * depth + FULL + i * q_part, 16), q_part),
            pl.ds(pl.multiple_of(x * quarter, quarter), quarter),
        ]

    def w_shard(s, first=0, size=depth):
        return wfull.at[pl.ds(pl.multiple_of(s * depth + first, 32), size)]

    steps = n_sp // 2
    owner = {"f": 0, "q": 1}

    def when_due(k, kind, action):
        if k < steps:
            action()
        elif k == steps:
            pl.when(c == owner[kind])(action)

    def z_send(part, k):
        ref = w_message(wrap(z - sign * k, n_sp), *part)
        row = parts.index(part)
        send(ref, ref, onward, wsend.at[row], wz_sem.at[row, k])

    def z_arrive(part, k):
        kind, i = part
        s = wrap(z - sign * k, n_sp)
        arrived(w_message(s, *part), wz_sem.at[parts.index(part), k - 1])
        when_due(k + 1, kind, functools.partial(z_send, part, k))
        if kind == "q" and i == PARTS[0] - 1:
            ref = w_part(s, x)
            send(ref, ref, ahead, wsend.at[WX], wx_sem.at[0, k - 1])
            send(ref, ref, behind, wsend.at[WX + 1], wx_sem.at[1, k - 1])

    def x_arrive(k):
        s = wrap(z - sign * k, n_sp)
        from_behind = w_part(s, wrap(x - sign, n_x))
        arrived(from_behind, wx_sem.at[0, k - 1])
        send(from_behind, from_behind, ahead, wsend.at[WX + 2], wx_sem.at[2, k - 1])
        arrived(w_part(s, wrap(x + sign, n_x)), wx_sem.at[1, k - 1])

    def hand_over(ref, k):
        send(ref, ref, partner, wsend.at[WX + 3], wp_sem.at[k - 1])

    def far_arrive(k):
        s = wrap(z - sign * k, n_sp)
        arrived(w_part(s, wrap(x + 2, n_x)), wx_sem.at[2, k - 1])
        if k < steps:
            hand_over(w_shard(s), k)
        else:
            hand_over(w_shard(s, FULL, depth - FULL), k)

    loads[0].wait()
    if True:
        for part in parts:
            z_send(part, 0)

    loads[1].wait()
    loads[4].wait()
    loads[5].wait()
    loads[6].wait()

    def normalise(part, parts):
        @pl.loop(part * 2 * rows // 32 // parts, (part + 1) * 2 * rows // 32 // parts)
        def _(n):
            r = pl.ds(pl.multiple_of(n * 32, 32), 32)
            wide = norm[r, :].astype(jnp.float32)
            scale = lax.rsqrt(jnp.sum(wide * wide, axis=-1, keepdims=True) * (1.0 / width) + EPS)
            norm[r, :] = (wide * scale * gain_ref[...]).astype(jnp.bfloat16)

    def partial(s, first=False):
        @pl.loop(0, n_x)
        def _(n):
            cols = pl.ds(pl.multiple_of(n * quarter, quarter), quarter)
            term = jnp.dot(
                norm[:, pl.ds(pl.multiple_of(s * depth, depth), depth)],
                wfull[pl.ds(pl.multiple_of(s * depth, depth), depth), cols],
                preferred_element_type=jnp.float32,
            )
            acc[:, cols] = term if first else acc[:, cols] + term

    def finish(k):
        s = wrap(z + sign * k, n_sp)
        if k < steps:
            arrived(w_shard(s), wp_sem.at[k - 1])
            partial(wrap(z - sign * k, n_sp))
        else:
            pl.when(c == 0)(lambda: arrived(w_shard(s, FULL, depth - FULL), wp_sem.at[k - 1]))
            pl.when(c == 1)(lambda: arrived(w_shard(s, 0, FULL), wp_sem.at[k - 1]))
        partial(s)

    def rotary():
        raw = lax.dot_general(
            wrope_ref[...], norm[...], (((1,), (1,)), ((), ())), preferred_element_type=jnp.float32
        )
        index = lax.broadcasted_iota(jnp.int32, (ROPE // 2, rows), 0).astype(jnp.float32) * 2.0
        inverse = jnp.exp(index * (-jnp.log(jnp.float32(10000.0)) / ROPE))
        place = lax.broadcasted_iota(jnp.int32, (ROPE // 2, rows), 1)
        for j in range(2):
            angle = (off_ref[j] + z * rows + place).astype(jnp.float32) * inverse
            cosine, sine = jnp.cos(angle), jnp.sin(angle)
            first = raw[: ROPE // 2, j * rows:(j + 1) * rows]
            second = raw[ROPE // 2:, j * rows:(j + 1) * rows]
            ropeown[j] = jnp.concatenate(
                [first * cosine - second * sine, second * cosine + first * sine], axis=0
            ).astype(jnp.bfloat16)

    def follow(k):
        for lag, action in zip(LAGS, (x_arrive, far_arrive, finish)):
            if 1 <= k - lag <= steps:
                step = functools.partial(action, k - lag)
                if action is finish:
                    step()
                else:
                    when_due(k - lag, "q", step)
        if k == 3:
            partial(z, True)
        if k == 4:
            rotary()

    normalise(0, 4)
    for k in range(1, steps + 1):
        for part in parts:
            when_due(k, part[0], functools.partial(z_arrive, part, k))
        if k == steps:
            pl.when(c == 0)(lambda: hand_over(w_shard(wrap(z + steps, n_sp), 0, FULL), steps))
        if k < 4:
            normalise(k, 4)
        follow(k)
    for k in range(steps + 1, steps + LAGS[2] + 1):
        follow(k)

    for j in range(2):
        own = jnp.logical_and(rope_self, 2 * t + j == z)
        dst = rope_ref.at[:, pl.ds(pl.multiple_of(z * rows, rows), rows)]

        @pl.when(own)
        def _():
            pltpu.make_async_copy(ropeown.at[j], dst, rsem.at[z]).start()

        @pl.when(jnp.logical_not(own))
        def _():
            send(ropeown.at[j], dst, dev(column, home, 2 * t + j), rsend.at[0, j], rsem.at[z])

    small = piece // HALVES

    def own_piece(j, q, h):
        return lat.at[pl.ds(pl.multiple_of(j * rows + (h * n_x + q) * small, small), small)]

    def staged(xx, j, h):
        return stage.at[xx, j, pl.ds(h * small, small)]

    def place_of(s, q, h):
        return latall.at[pl.ds(pl.multiple_of(s * rows + (h * n_x + q) * small, small), small)]

    @pl.loop(0, 2 * rows // 64)
    def _(n):
        r = pl.ds(pl.multiple_of(n * 64, 64), 64)
        wide = acc[r, :]
        scale = lax.rsqrt(jnp.sum(wide * wide, axis=-1, keepdims=True) * (1.0 / rank) + EPS)
        lat[r, :] = (wide * scale * kvg_ref[...]).astype(jnp.bfloat16)

    for h in range(HALVES):
        for j in range(2):
            for d in (2, 1, -1):
                q = wrap(x + d, n_x)
                send(own_piece(j, q, h), staged(x, j, h), dev(q, c, z), lsend.at[0, j], a_sem.at[x, j, h])
    for h in range(HALVES):
        for j in range(2):
            stage[x, j, pl.ds(h * small, small)] = lat[
                pl.ds(pl.multiple_of(j * rows + (h * n_x + x) * small, small), small), :
            ]

    origin = lax.rem(z - 2 * c + n_sp, n_sp) // 4
    for h in range(HALVES):
        for d in (0, 1, -1, 2):
            xx = wrap(origin + d, n_x)
            for j in range(2):
                goal = 4 * xx + 2 * c + j
                own = jnp.logical_and(has_self, goal == z)

                @pl.when(xx != x)
                def _():
                    arrived(staged(xx, j, h), a_sem.at[xx, j, h])

                src, dst, sem = staged(xx, j, h), place_of(z, x, h), dir_sem.at[z // 2, h]

                @pl.when(own)
                def _():
                    pltpu.make_async_copy(src, dst, sem).start()

                @pl.when(jnp.logical_not(own))
                def _():
                    send(src, dst, dev(x, home, goal), lsend.at[3, 0], sem)

    near = [0] + [v for k in range(2, steps, 2) for v in (k, -k)] + [steps]
    odd = [v for k in range(1, steps, 2) for v in (k, -k)]
    same = home == c
    sources = [wrap(z + jnp.where(same, a, b), n_sp) for a, b in zip(near, odd)]
    other = [wrap(z + jnp.where(same, b, a), n_sp) for a, b in zip(near, odd)]
    n_src = len(sources)

    def direct(n, h):
        s = sources[n]
        ref = place_of(s, x, h)
        arrived(ref, dir_sem.at[s // 2, h])
        send(ref, ref, right, lsend.at[1, 0], lx_sem.at[0, n, h])
        send(ref, ref, left, lsend.at[1, 1], lx_sem.at[1, n, h])

    def beside(n, h):
        s = sources[n]
        from_left, from_right = place_of(s, wrap(x - 1, n_x), h), place_of(s, wrap(x + 1, n_x), h)
        arrived(from_left, lx_sem.at[0, n, h])
        if (n + h) % 2 == 0:
            send(from_left, from_left, right, lsend.at[2, 0], lx_sem.at[2, n, h])
        arrived(from_right, lx_sem.at[1, n, h])
        if (n + h) % 2 == 1:
            send(from_right, from_right, left, lsend.at[2, 0], lx_sem.at[2, n, h])

    def block(s, h):
        return latall.at[pl.ds(pl.multiple_of(s * rows + h * n_x * small, small), n_x * small)]

    def far(n, h):
        s = sources[n]
        arrived(place_of(s, wrap(x + 2, n_x), h), lx_sem.at[2, n, h])
        send(block(s, h), block(s, h), partner, lsend.at[2, 1], lp_sem.at[s, h])

    def up_project(s, h):
        r = pl.ds(pl.multiple_of(s * rows + h * n_x * small, small), n_x * small)
        both = jnp.dot(latall[r, :], wup[...], preferred_element_type=jnp.float32).astype(jnp.bfloat16)
        keys_ref[r, :] = both[:, :heads]
        values_ref[r, :] = both[:, heads:]

    def rope_block(s):
        return rope_ref.at[:, pl.ds(pl.multiple_of(s * rows, rows), rows)]

    peers = [(dx, dc) for dx in range(n_x) for dc in range(2) if dx or dc]
    def rope_onward():
        for g in range(n_sp // 2 // n_x):
            s = 2 * (x + n_x * g) + c
            arrived(rope_block(s), rsem.at[s])
            for n, (dx, dc) in enumerate(peers):
                send(
                    rope_block(s), rope_block(s), dev(wrap(x + dx, n_x), lax.rem(c + dc, 2), z),
                    rsend.at[1 + g, n], rsem.at[s],
                )

    loads[2].wait()
    loads[3].wait()
    order = [(n, h) for h in range(HALVES) for n in range(n_src)]

    def other_half(n, h):
        s = other[n]
        arrived(block(s, h), lp_sem.at[s, h])
        up_project(s, h)

    def far_half(n, h):
        far(n, h)
        up_project(sources[n], h)

    actions = ((0, direct), (2, beside), (5, far_half), (6, other_half))
    for i in range(len(order) + 6):
        for lag, action in actions:
            if 0 <= i - lag < len(order):
                action(*order[i - lag])
        if i == 6:
            rope_onward()

    for s in range(n_sp):
        mine = jnp.logical_and(lax.rem(s // 2, n_x) == x, s % 2 == c)

        @pl.when(jnp.logical_not(mine))
        def _():
            arrived(rope_block(s), rsem.at[s])

    for j in range(2):
        own = jnp.logical_and(rope_self, 2 * t + j == z)

        @pl.when(jnp.logical_not(own))
        def _():
            arrived(ropeown.at[j], rsend.at[0, j])

    for g in range(n_sp // 2 // n_x):
        for n in range(len(peers)):
            arrived(ropeown.at[0], rsend.at[1 + g, n])
    for core in range(2):
        @pl.when(c == core)
        def _():
            trips = {kind: steps - (owner[kind] != core) for kind in owner}
            for row, (kind, _) in enumerate(parts):
                if kind == "f":
                    arrived(wfull.at[pl.ds(0, trips[kind] * f_part)], wsend.at[row])
                else:
                    arrived(wfull.at[pl.ds(0, trips[kind] * q_part), pl.ds(0, quarter)], wsend.at[row])
            for row in range(WX, WX + 3):
                arrived(wfull.at[pl.ds(0, trips["q"] * (depth - FULL)), pl.ds(0, quarter)], wsend.at[row])
            last = FULL if core == 0 else depth - FULL
            arrived(wfull.at[pl.ds(0, (steps - 1) * depth + last)], wsend.at[WX + 3])

    if True:
        for j in range(2):
            arrived(lat.at[pl.ds(0, rows - piece)], lsend.at[0, j])
        pl.when(has_self)(lambda: arrived(lat.at[pl.ds(0, 2 * rows - piece)], lsend.at[3, 0]))
        pl.when(jnp.logical_not(has_self))(lambda: arrived(lat, lsend.at[3, 0]))
        for a, b in ((1, 0), (1, 1), (2, 0)):
            arrived(latall.at[pl.ds(0, n_src * piece)], lsend.at[a, b])
        arrived(latall.at[pl.ds(0, n_src * rows)], lsend.at[2, 1])


def in_hbm(value):
    return pltpu.with_memory_space_constraint(value, pltpu.HBM)


def attend(
    keys_ref, values_ref, rope_ref, qn_ref, qr_ref, keys_out, values_out, rope_out, read_ref, sem
):
    outs = [
        pltpu.make_async_copy(keys_ref, keys_out, sem.at[0]),
        pltpu.make_async_copy(values_ref, values_out, sem.at[1]),
        pltpu.make_async_copy(rope_ref, rope_out, sem.at[2]),
    ]
    for out in outs:
        out.start()
    heads = keys_ref.shape[1] // HEAD
    rot = qr_ref.shape[1] // heads
    pad = 8

    def by_head(ref, size):
        wide = jnp.broadcast_to(ref[...].astype(jnp.float32), (pad, ref.shape[1]))
        row = lax.broadcasted_iota(jnp.int32, wide.shape, 0)
        col = lax.broadcasted_iota(jnp.int32, wide.shape, 1)
        return jnp.where(col // size == row, wide, 0.0)

    nope = by_head(qn_ref, HEAD).astype(jnp.bfloat16)
    scores = lax.dot_general(
        nope, keys_ref[...], (((1,), (1,)), ((), ())), preferred_element_type=jnp.float32
    )
    spread = by_head(qr_ref, rot)
    rotary = spread[:, :rot]
    for h in range(1, heads):
        rotary = rotary + spread[:, h * rot:(h + 1) * rot]
    scores = scores + jnp.dot(
        rotary.astype(jnp.bfloat16), rope_ref[...], preferred_element_type=jnp.float32
    )
    scores = scores / jnp.sqrt(jnp.float32(HEAD + ROPE))
    expo = jnp.exp(scores - jnp.max(scores, axis=-1, keepdims=True))
    weights = (expo / jnp.sum(expo, axis=-1, keepdims=True)).astype(jnp.bfloat16)
    read = jnp.dot(weights, values_ref[...], preferred_element_type=jnp.float32)
    row = lax.broadcasted_iota(jnp.int32, read.shape, 0)
    col = lax.broadcasted_iota(jnp.int32, read.shape, 1)
    read_ref[...] = jnp.sum(
        jnp.where(col // HEAD == row, read, 0.0), axis=0, keepdims=True
    ).astype(jnp.bfloat16)
    for out in outs:
        out.wait()


def local(
    n_sp, n_tp,
    tokens, offsets, in_gain, w_latent, w_rope_key, kv_gain, w_up_key, w_up_value, q_nope, q_rope
):
    prompts, rows, width = tokens.shape
    depth, rank = w_latent.shape
    heads = w_up_key.shape[1]
    length = n_sp * rows
    steps = n_sp // 2
    any_space = pl.BlockSpec(memory_space=pl.ANY)
    hbm = pl.BlockSpec(memory_space=pltpu.HBM)
    vmem = pl.BlockSpec(memory_space=pltpu.VMEM)
    smem = pl.BlockSpec(memory_space=pltpu.SMEM)
    dma = pltpu.SemaphoreType.DMA
    keys, values, rope = pl.pallas_call(
        functools.partial(exchange, n_sp, n_tp),
        out_shape=(
            jax.ShapeDtypeStruct((length, heads), jnp.bfloat16),
            jax.ShapeDtypeStruct((length, heads), jnp.bfloat16),
            jax.ShapeDtypeStruct((ROPE, length), jnp.bfloat16),
        ),
        in_specs=[hbm, smem, hbm, hbm, hbm, hbm, hbm, hbm],
        out_specs=(vmem, vmem, vmem),
        scratch_shapes=[
            pltpu.VMEM((prompts * rows, width), jnp.bfloat16),
            pltpu.VMEM((width, rank), jnp.bfloat16),
            pltpu.VMEM((rank, 2 * heads), jnp.bfloat16),
            pltpu.VMEM((prompts * rows, rank), jnp.bfloat16),
            pltpu.VMEM((prompts * rows, rank), jnp.float32),
            pltpu.VMEM((length, rank), jnp.bfloat16),
            pltpu.VMEM((prompts, ROPE, rows), jnp.bfloat16),
            pltpu.VMEM((n_tp // 2, prompts, rows * 2 // n_tp, rank), jnp.bfloat16),
            pltpu.VMEM((1, width), jnp.float32),
            pltpu.VMEM((ROPE, width), jnp.bfloat16),
            pltpu.VMEM((1, rank), jnp.float32),
            dma((7,)),
            dma((WX, steps)),
            dma((3, steps)),
            dma((steps,)),
            dma((WX + 4,)),
            dma((n_tp // 2, prompts, HALVES)),
            dma((steps, HALVES)),
            dma((3, steps, HALVES)),
            dma((n_sp, HALVES)),
            dma((4, 2)),
            dma((n_sp,)),
            dma((1 + n_sp // n_tp, n_tp - 1)),
        ],
        compiler_params=pltpu.CompilerParams(
            collective_id=0, has_side_effects=True, vmem_limit_bytes=40 * 1024 * 1024
        ),
        name="exchange",
    )(
        *map(
            in_hbm,
            (tokens.reshape(prompts * rows, width),),
        ),
        offsets,
        *map(
            in_hbm,
            (
                in_gain.reshape(1, width), w_latent, w_rope_key.T, kv_gain.reshape(1, rank),
                w_up_key, w_up_value,
            ),
        ),
    )
    return pl.pallas_call(
        attend,
        out_shape=(
            jax.ShapeDtypeStruct((length, heads), jnp.bfloat16),
            jax.ShapeDtypeStruct((length, heads), jnp.bfloat16),
            jax.ShapeDtypeStruct((ROPE, length), jnp.bfloat16),
            jax.ShapeDtypeStruct((1, heads), jnp.bfloat16),
        ),
        in_specs=[vmem] * 5,
        out_specs=(any_space, any_space, any_space, vmem),
        scratch_shapes=[dma((3,))],
        compiler_params=pltpu.CompilerParams(vmem_limit_bytes=24 * 1024 * 1024),
        name="attend",
    )(keys, values, rope, q_nope, q_rope)


def solution(mesh):
    n_sp, n_tp = mesh.shape["sp"], mesh.shape["tp"]

    def body(*args):
        keys, values, rope, read = local(n_sp, n_tp, *args)
        return keys[None], values[None], rope[None], read

    in_specs = (
        P(("grp", "tp"), "sp", None),
        P(("grp", "tp")),
        P(),
        P("sp", None),
        P(),
        P(),
        P(None, "tp"),
        P(None, "tp"),
        P(("grp", "sp"), "tp"),
        P(("grp", "sp"), "tp"),
    )
    out_specs = (
        P(("grp", "sp"), None, "tp"),
        P(("grp", "sp"), None, "tp"),
        P(("grp", "sp"), None, None),
        P(("grp", "sp"), "tp"),
    )
    return jax.shard_map(body, mesh=mesh, in_specs=in_specs, out_specs=out_specs, check_vma=False)
```

```python
import functools

import jax
import jax.numpy as jnp
from jax import lax
from jax.experimental import pallas as pl
from jax.experimental.pallas import tpu as pltpu
from jax.sharding import PartitionSpec as P

HEAD = 64
ROPE = 32
EPS = 1e-06
MESH = pl.DeviceIdType.MESH
WX = 5
FULL = 96

LAGS = (1, 3, 4)
HALVES = 2
PARTS = (2, 3)


def exchange(
    n_sp, n_tp, tok_hbm, off_ref, gain_hbm, wl_hbm, wrope_hbm, kvg_hbm, wk_hbm, wv_hbm,
    keys_ref, values_ref, rope_ref,
    norm, wfull, wup, lat, acc, latall, ropeown, stage, gain_ref, wrope_ref, kvg_ref,
    local_sem, wz_sem, wx_sem, wp_sem, wsend, a_sem, dir_sem, lx_sem, lp_sem, lsend, rsem, rsend,
):
    z = lax.axis_index("sp")
    t = lax.axis_index("tp")
    n_x = n_tp // 2
    x, c = t // 2, lax.rem(t, 2)
    rows = norm.shape[0] // 2
    width = norm.shape[1]
    rank = lat.shape[1]
    depth = width // n_sp
    quarter = rank // n_x
    piece = rows // n_x
    heads = keys_ref.shape[1]

    def wrap(v, n):
        return lax.rem(v + 2 * n, n)

    def dev(xx, cc, zz):
        return {"sp": zz, "tp": 2 * xx + cc}

    z_next, z_prev = wrap(z + 1, n_sp), wrap(z - 1, n_sp)
    right = dev(wrap(x + 1, n_x), c, z)
    left = dev(wrap(x - 1, n_x), c, z)
    up = dev(x, c, z_next)
    down = dev(x, c, z_prev)
    partner = dev(x, 1 - c, z)
    home = lax.rem(z, 2)
    src_x, src_c = z // 4, lax.rem(z // 2, 2)
    has_self = jnp.logical_and(src_c == c, c == home)

    loads = [
        pltpu.make_async_copy(wl_hbm, wfull.at[pl.ds(z * depth, depth)], local_sem.at[0]),
        pltpu.make_async_copy(tok_hbm, norm, local_sem.at[1]),
        pltpu.make_async_copy(wk_hbm, wup.at[:, pl.ds(0, heads)], local_sem.at[2]),
        pltpu.make_async_copy(wv_hbm, wup.at[:, pl.ds(heads, heads)], local_sem.at[3]),
        pltpu.make_async_copy(gain_hbm, gain_ref, local_sem.at[4]),
        pltpu.make_async_copy(wrope_hbm, wrope_ref, local_sem.at[5]),
        pltpu.make_async_copy(kvg_hbm, kvg_ref, local_sem.at[6]),
    ]
    for load in loads:
        load.start()

    barrier = pltpu.get_barrier_semaphore()

    def greet(device):
        pl.semaphore_signal(barrier, inc=1, device_id=device, device_id_type=MESH)

    column = lax.rem(z // 2, n_x)
    rope_self = jnp.logical_and(jnp.logical_and(x == src_x, c == src_c), jnp.logical_and(x == column, c == home))
    around = (right, left, up, down, partner)
    for device in around:
        greet(device)
    pl.semaphore_wait(barrier, len(around))

    def send(src, dst, device, send_sem, recv_sem):
        pltpu.make_async_remote_copy(
            src_ref=src, dst_ref=dst, send_sem=send_sem, recv_sem=recv_sem,
            device_id=device, device_id_type=MESH,
        ).start()

    def arrived(dst, recv_sem):
        pltpu.make_async_copy(dst, dst, recv_sem).wait()

    sign = 1 - 2 * c
    onward = dev(x, c, wrap(z + sign, n_sp))
    ahead, behind = dev(wrap(x + sign, n_x), c, z), dev(wrap(x - sign, n_x), c, z)
    q_part, f_part = (depth - FULL) // PARTS[0], FULL // PARTS[1]
    parts = [("q", i) for i in range(PARTS[0])] + [("f", i) for i in range(PARTS[1])]

    def w_part(s, xx):
        return wfull.at[
            pl.ds(pl.multiple_of(s * depth + FULL, 32), depth - FULL),
            pl.ds(pl.multiple_of(xx * quarter, quarter), quarter),
        ]

    def w_message(s, kind, i):
        if kind == "f":
            return wfull.at[pl.ds(pl.multiple_of(s * depth + i * f_part, f_part), f_part)]
        return wfull.at[
            pl.ds(pl.multiple_of(s * depth + FULL + i * q_part, 16), q_part),
            pl.ds(pl.multiple_of(x * quarter, quarter), quarter),
        ]

    def w_shard(s, first=0, size=depth):
        return wfull.at[pl.ds(pl.multiple_of(s * depth + first, 32), size)]

    steps = n_sp // 2
    owner = {"f": 0, "q": 1}

    def when_due(k, kind, action):
        if k < steps:
            action()
        elif k == steps:
            pl.when(c == owner[kind])(action)

    def z_send(part, k):
        ref = w_message(wrap(z - sign * k, n_sp), *part)
        row = parts.index(part)
        send(ref, ref, onward, wsend.at[row], wz_sem.at[row, k])

    def z_arrive(part, k):
        kind, i = part
        s = wrap(z - sign * k, n_sp)
        arrived(w_message(s, *part), wz_sem.at[parts.index(part), k - 1])
        when_due(k + 1, kind, functools.partial(z_send, part, k))
        if kind == "q" and i == PARTS[0] - 1:
            ref = w_part(s, x)
            send(ref, ref, ahead, wsend.at[WX], wx_sem.at[0, k - 1])
            send(ref, ref, behind, wsend.at[WX + 1], wx_sem.at[1, k - 1])

    def x_arrive(k):
        s = wrap(z - sign * k, n_sp)
        from_behind = w_part(s, wrap(x - sign, n_x))
        arrived(from_behind, wx_sem.at[0, k - 1])
        send(from_behind, from_behind, ahead, wsend.at[WX + 2], wx_sem.at[2, k - 1])
        arrived(w_part(s, wrap(x + sign, n_x)), wx_sem.at[1, k - 1])

    def hand_over(ref, k):
        send(ref, ref, partner, wsend.at[WX + 3], wp_sem.at[k - 1])

    def far_arrive(k):
        s = wrap(z - sign * k, n_sp)
        arrived(w_part(s, wrap(x + 2, n_x)), wx_sem.at[2, k - 1])
        if k < steps:
            hand_over(w_shard(s), k)
        else:
            hand_over(w_shard(s, FULL, depth - FULL), k)

    loads[0].wait()
    if True:
        for part in parts:
            z_send(part, 0)

    loads[1].wait()
    loads[4].wait()
    loads[5].wait()
    loads[6].wait()

    def normalise(part, parts):
        @pl.loop(part * 2 * rows // 32 // parts, (part + 1) * 2 * rows // 32 // parts)
        def _(n):
            r = pl.ds(pl.multiple_of(n * 32, 32), 32)
            wide = norm[r, :].astype(jnp.float32)
            scale = lax.rsqrt(jnp.sum(wide * wide, axis=-1, keepdims=True) * (1.0 / width) + EPS)
            norm[r, :] = (wide * scale * gain_ref[...]).astype(jnp.bfloat16)

    def partial(s, first=False):
        @pl.loop(0, n_x)
        def _(n):
            cols = pl.ds(pl.multiple_of(n * quarter, quarter), quarter)
            term = jnp.dot(
                norm[:, pl.ds(pl.multiple_of(s * depth, depth), depth)],
                wfull[pl.ds(pl.multiple_of(s * depth, depth), depth), cols],
                preferred_element_type=jnp.float32,
            )
            acc[:, cols] = term if first else acc[:, cols] + term

    def finish(k):
        s = wrap(z + sign * k, n_sp)
        if k < steps:
            arrived(w_shard(s), wp_sem.at[k - 1])
            partial(wrap(z - sign * k, n_sp))
        else:
            pl.when(c == 0)(lambda: arrived(w_shard(s, FULL, depth - FULL), wp_sem.at[k - 1]))
            pl.when(c == 1)(lambda: arrived(w_shard(s, 0, FULL), wp_sem.at[k - 1]))
        partial(s)

    def rotary():
        raw = lax.dot_general(
            wrope_ref[...], norm[...], (((1,), (1,)), ((), ())), preferred_element_type=jnp.float32
        )
        index = lax.broadcasted_iota(jnp.int32, (ROPE // 2, rows), 0).astype(jnp.float32) * 2.0
        inverse = jnp.exp(index * (-jnp.log(jnp.float32(10000.0)) / ROPE))
        place = lax.broadcasted_iota(jnp.int32, (ROPE // 2, rows), 1)
        for j in range(2):
            angle = (off_ref[j] + z * rows + place).astype(jnp.float32) * inverse
            cosine, sine = jnp.cos(angle), jnp.sin(angle)
            first = raw[: ROPE // 2, j * rows:(j + 1) * rows]
            second = raw[ROPE // 2:, j * rows:(j + 1) * rows]
            ropeown[j] = jnp.concatenate(
                [first * cosine - second * sine, second * cosine + first * sine], axis=0
            ).astype(jnp.bfloat16)

    def follow(k):
        for lag, action in zip(LAGS, (x_arrive, far_arrive, finish)):
            if 1 <= k - lag <= steps:
                step = functools.partial(action, k - lag)
                if action is finish:
                    step()
                else:
                    when_due(k - lag, "q", step)
        if k == 3:
            partial(z, True)
        if k == 4:
            rotary()

    normalise(0, 4)
    for k in range(1, steps + 1):
        for part in parts:
            when_due(k, part[0], functools.partial(z_arrive, part, k))
        if k == steps:
            pl.when(c == 0)(lambda: hand_over(w_shard(wrap(z + steps, n_sp), 0, FULL), steps))
        if k < 4:
            normalise(k, 4)
        follow(k)
    for k in range(steps + 1, steps + LAGS[2] + 1):
        follow(k)

    for j in range(2):
        own = jnp.logical_and(rope_self, 2 * t + j == z)
        dst = rope_ref.at[:, pl.ds(pl.multiple_of(z * rows, rows), rows)]

        @pl.when(own)
        def _():
            pltpu.make_async_copy(ropeown.at[j], dst, rsem.at[z]).start()

        @pl.when(jnp.logical_not(own))
        def _():
            send(ropeown.at[j], dst, dev(column, home, 2 * t + j), rsend.at[0, j], rsem.at[z])

    small = piece // HALVES

    def own_piece(j, q, h):
        return lat.at[pl.ds(pl.multiple_of(j * rows + (h * n_x + q) * small, small), small)]

    def staged(xx, j, h):
        return stage.at[xx, j, pl.ds(h * small, small)]

    def place_of(s, q, h):
        return latall.at[pl.ds(pl.multiple_of(s * rows + (h * n_x + q) * small, small), small)]

    @pl.loop(0, 2 * rows // 64)
    def _(n):
        r = pl.ds(pl.multiple_of(n * 64, 64), 64)
        wide = acc[r, :]
        scale = lax.rsqrt(jnp.sum(wide * wide, axis=-1, keepdims=True) * (1.0 / rank) + EPS)
        lat[r, :] = (wide * scale * kvg_ref[...]).astype(jnp.bfloat16)

    for h in range(HALVES):
        for j in range(2):
            for d in (2, 1, -1):
                q = wrap(x + d, n_x)
                send(own_piece(j, q, h), staged(x, j, h), dev(q, c, z), lsend.at[0, j], a_sem.at[x, j, h])
    for h in range(HALVES):
        for j in range(2):
            stage[x, j, pl.ds(h * small, small)] = lat[
                pl.ds(pl.multiple_of(j * rows + (h * n_x + x) * small, small), small), :
            ]

    origin = lax.rem(z - 2 * c + n_sp, n_sp) // 4
    for h in range(HALVES):
        for d in (0, 1, -1, 2):
            xx = wrap(origin + d, n_x)
            for j in range(2):
                goal = 4 * xx + 2 * c + j
                own = jnp.logical_and(has_self, goal == z)

                @pl.when(xx != x)
                def _():
                    arrived(staged(xx, j, h), a_sem.at[xx, j, h])

                src, dst, sem = staged(xx, j, h), place_of(z, x, h), dir_sem.at[z // 2, h]

                @pl.when(own)
                def _():
                    pltpu.make_async_copy(src, dst, sem).start()

                @pl.when(jnp.logical_not(own))
                def _():
                    send(src, dst, dev(x, home, goal), lsend.at[3, 0], sem)

    near = [0] + [v for k in range(2, steps, 2) for v in (k, -k)] + [steps]
    odd = [v for k in range(1, steps, 2) for v in (k, -k)]
    same = home == c
    sources = [wrap(z + jnp.where(same, a, b), n_sp) for a, b in zip(near, odd)]
    other = [wrap(z + jnp.where(same, b, a), n_sp) for a, b in zip(near, odd)]
    n_src = len(sources)

    def direct(n, h):
        s = sources[n]
        ref = place_of(s, x, h)
        arrived(ref, dir_sem.at[s // 2, h])
        send(ref, ref, right, lsend.at[1, 0], lx_sem.at[0, n, h])
        send(ref, ref, left, lsend.at[1, 1], lx_sem.at[1, n, h])

    def beside(n, h):
        s = sources[n]
        from_left, from_right = place_of(s, wrap(x - 1, n_x), h), place_of(s, wrap(x + 1, n_x), h)
        arrived(from_left, lx_sem.at[0, n, h])
        if (n + h) % 2 == 0:
            send(from_left, from_left, right, lsend.at[2, 0], lx_sem.at[2, n, h])
        arrived(from_right, lx_sem.at[1, n, h])
        if (n + h) % 2 == 1:
            send(from_right, from_right, left, lsend.at[2, 0], lx_sem.at[2, n, h])

    def block(s, h):
        return latall.at[pl.ds(pl.multiple_of(s * rows + h * n_x * small, small), n_x * small)]

    def far(n, h):
        s = sources[n]
        arrived(place_of(s, wrap(x + 2, n_x), h), lx_sem.at[2, n, h])
        send(block(s, h), block(s, h), partner, lsend.at[2, 1], lp_sem.at[s, h])

    def up_project(s, h):
        r = pl.ds(pl.multiple_of(s * rows + h * n_x * small, small), n_x * small)
        both = jnp.dot(latall[r, :], wup[...], preferred_element_type=jnp.float32).astype(jnp.bfloat16)
        keys_ref[r, :] = both[:, :heads]
        values_ref[r, :] = both[:, heads:]

    def rope_block(s):
        return rope_ref.at[:, pl.ds(pl.multiple_of(s * rows, rows), rows)]

    peers = [(dx, dc) for dx in range(n_x) for dc in range(2) if dx or dc]
    def rope_onward():
        for g in range(n_sp // 2 // n_x):
            s = 2 * (x + n_x * g) + c
            arrived(rope_block(s), rsem.at[s])
            for n, (dx, dc) in enumerate(peers):
                send(
                    rope_block(s), rope_block(s), dev(wrap(x + dx, n_x), lax.rem(c + dc, 2), z),
                    rsend.at[1 + g, n], rsem.at[s],
                )

    loads[2].wait()
    loads[3].wait()
    order = [(n, h) for h in range(HALVES) for n in range(n_src)]

    def other_half(n, h):
        s = other[n]
        arrived(block(s, h), lp_sem.at[s, h])
        up_project(s, h)

    def far_half(n, h):
        far(n, h)
        up_project(sources[n], h)

    actions = ((0, direct), (3, beside), (6, far_half), (8, other_half))
    for i in range(len(order) + 8):
        for lag, action in actions:
            if 0 <= i - lag < len(order):
                action(*order[i - lag])
        if i == 9:
            rope_onward()

    for s in range(n_sp):
        mine = jnp.logical_and(lax.rem(s // 2, n_x) == x, s % 2 == c)

        @pl.when(jnp.logical_not(mine))
        def _():
            arrived(rope_block(s), rsem.at[s])

    for j in range(2):
        own = jnp.logical_and(rope_self, 2 * t + j == z)

        @pl.when(jnp.logical_not(own))
        def _():
            arrived(ropeown.at[j], rsend.at[0, j])

    for g in range(n_sp // 2 // n_x):
        for n in range(len(peers)):
            arrived(ropeown.at[0], rsend.at[1 + g, n])
    for core in range(2):
        @pl.when(c == core)
        def _():
            trips = {kind: steps - (owner[kind] != core) for kind in owner}
            for row, (kind, _) in enumerate(parts):
                if kind == "f":
                    arrived(wfull.at[pl.ds(0, trips[kind] * f_part)], wsend.at[row])
                else:
                    arrived(wfull.at[pl.ds(0, trips[kind] * q_part), pl.ds(0, quarter)], wsend.at[row])
            for row in range(WX, WX + 3):
                arrived(wfull.at[pl.ds(0, trips["q"] * (depth - FULL)), pl.ds(0, quarter)], wsend.at[row])
            last = FULL if core == 0 else depth - FULL
            arrived(wfull.at[pl.ds(0, (steps - 1) * depth + last)], wsend.at[WX + 3])

    if True:
        for j in range(2):
            arrived(lat.at[pl.ds(0, rows - piece)], lsend.at[0, j])
        pl.when(has_self)(lambda: arrived(lat.at[pl.ds(0, 2 * rows - piece)], lsend.at[3, 0]))
        pl.when(jnp.logical_not(has_self))(lambda: arrived(lat, lsend.at[3, 0]))
        for a, b in ((1, 0), (1, 1), (2, 0)):
            arrived(latall.at[pl.ds(0, n_src * piece)], lsend.at[a, b])
        arrived(latall.at[pl.ds(0, n_src * rows)], lsend.at[2, 1])


def in_hbm(value):
    return pltpu.with_memory_space_constraint(value, pltpu.HBM)


def attend(
    keys_ref, values_ref, rope_ref, qn_ref, qr_ref, keys_out, values_out, rope_out, read_ref, sem
):
    outs = [
        pltpu.make_async_copy(keys_ref, keys_out, sem.at[0]),
        pltpu.make_async_copy(values_ref, values_out, sem.at[1]),
        pltpu.make_async_copy(rope_ref, rope_out, sem.at[2]),
    ]
    for out in outs:
        out.start()
    heads = keys_ref.shape[1] // HEAD
    rot = qr_ref.shape[1] // heads
    pad = 8

    def by_head(ref, size):
        wide = jnp.broadcast_to(ref[...].astype(jnp.float32), (pad, ref.shape[1]))
        row = lax.broadcasted_iota(jnp.int32, wide.shape, 0)
        col = lax.broadcasted_iota(jnp.int32, wide.shape, 1)
        return jnp.where(col // size == row, wide, 0.0)

    nope = by_head(qn_ref, HEAD).astype(jnp.bfloat16)
    scores = lax.dot_general(
        nope, keys_ref[...], (((1,), (1,)), ((), ())), preferred_element_type=jnp.float32
    )
    spread = by_head(qr_ref, rot)
    rotary = spread[:, :rot]
    for h in range(1, heads):
        rotary = rotary + spread[:, h * rot:(h + 1) * rot]
    scores = scores + jnp.dot(
        rotary.astype(jnp.bfloat16), rope_ref[...], preferred_element_type=jnp.float32
    )
    scores = scores / jnp.sqrt(jnp.float32(HEAD + ROPE))
    expo = jnp.exp(scores - jnp.max(scores, axis=-1, keepdims=True))
    weights = (expo / jnp.sum(expo, axis=-1, keepdims=True)).astype(jnp.bfloat16)
    read = jnp.dot(weights, values_ref[...], preferred_element_type=jnp.float32)
    row = lax.broadcasted_iota(jnp.int32, read.shape, 0)
    col = lax.broadcasted_iota(jnp.int32, read.shape, 1)
    read_ref[...] = jnp.sum(
        jnp.where(col // HEAD == row, read, 0.0), axis=0, keepdims=True
    ).astype(jnp.bfloat16)
    for out in outs:
        out.wait()


def local(
    n_sp, n_tp,
    tokens, offsets, in_gain, w_latent, w_rope_key, kv_gain, w_up_key, w_up_value, q_nope, q_rope
):
    prompts, rows, width = tokens.shape
    depth, rank = w_latent.shape
    heads = w_up_key.shape[1]
    length = n_sp * rows
    steps = n_sp // 2
    any_space = pl.BlockSpec(memory_space=pl.ANY)
    hbm = pl.BlockSpec(memory_space=pltpu.HBM)
    vmem = pl.BlockSpec(memory_space=pltpu.VMEM)
    smem = pl.BlockSpec(memory_space=pltpu.SMEM)
    dma = pltpu.SemaphoreType.DMA
    keys, values, rope = pl.pallas_call(
        functools.partial(exchange, n_sp, n_tp),
        out_shape=(
            jax.ShapeDtypeStruct((length, heads), jnp.bfloat16),
            jax.ShapeDtypeStruct((length, heads), jnp.bfloat16),
            jax.ShapeDtypeStruct((ROPE, length), jnp.bfloat16),
        ),
        in_specs=[hbm, smem, hbm, hbm, hbm, hbm, hbm, hbm],
        out_specs=(vmem, vmem, vmem),
        scratch_shapes=[
            pltpu.VMEM((prompts * rows, width), jnp.bfloat16),
            pltpu.VMEM((width, rank), jnp.bfloat16),
            pltpu.VMEM((rank, 2 * heads), jnp.bfloat16),
            pltpu.VMEM((prompts * rows, rank), jnp.bfloat16),
            pltpu.VMEM((prompts * rows, rank), jnp.float32),
            pltpu.VMEM((length, rank), jnp.bfloat16),
            pltpu.VMEM((prompts, ROPE, rows), jnp.bfloat16),
            pltpu.VMEM((n_tp // 2, prompts, rows * 2 // n_tp, rank), jnp.bfloat16),
            pltpu.VMEM((1, width), jnp.float32),
            pltpu.VMEM((ROPE, width), jnp.bfloat16),
            pltpu.VMEM((1, rank), jnp.float32),
            dma((7,)),
            dma((WX, steps)),
            dma((3, steps)),
            dma((steps,)),
            dma((WX + 4,)),
            dma((n_tp // 2, prompts, HALVES)),
            dma((steps, HALVES)),
            dma((3, steps, HALVES)),
            dma((n_sp, HALVES)),
            dma((4, 2)),
            dma((n_sp,)),
            dma((1 + n_sp // n_tp, n_tp - 1)),
        ],
        compiler_params=pltpu.CompilerParams(
            collective_id=0, has_side_effects=True, vmem_limit_bytes=40 * 1024 * 1024
        ),
        name="exchange",
    )(
        *map(
            in_hbm,
            (tokens.reshape(prompts * rows, width),),
        ),
        offsets,
        *map(
            in_hbm,
            (
                in_gain.reshape(1, width), w_latent, w_rope_key.T, kv_gain.reshape(1, rank),
                w_up_key, w_up_value,
            ),
        ),
    )
    return pl.pallas_call(
        attend,
        out_shape=(
            jax.ShapeDtypeStruct((length, heads), jnp.bfloat16),
            jax.ShapeDtypeStruct((length, heads), jnp.bfloat16),
            jax.ShapeDtypeStruct((ROPE, length), jnp.bfloat16),
            jax.ShapeDtypeStruct((1, heads), jnp.bfloat16),
        ),
        in_specs=[vmem] * 5,
        out_specs=(any_space, any_space, any_space, vmem),
        scratch_shapes=[dma((3,))],
        compiler_params=pltpu.CompilerParams(vmem_limit_bytes=24 * 1024 * 1024),
        name="attend",
    )(keys, values, rope, q_nope, q_rope)


def solution(mesh):
    n_sp, n_tp = mesh.shape["sp"], mesh.shape["tp"]

    def body(*args):
        keys, values, rope, read = local(n_sp, n_tp, *args)
        return keys[None], values[None], rope[None], read

    in_specs = (
        P(("grp", "tp"), "sp", None),
        P(("grp", "tp")),
        P(),
        P("sp", None),
        P(),
        P(),
        P(None, "tp"),
        P(None, "tp"),
        P(("grp", "sp"), "tp"),
        P(("grp", "sp"), "tp"),
    )
    out_specs = (
        P(("grp", "sp"), None, "tp"),
        P(("grp", "sp"), None, "tp"),
        P(("grp", "sp"), None, None),
        P(("grp", "sp"), "tp"),
    )
    return jax.shard_map(body, mesh=mesh, in_specs=in_specs, out_specs=out_specs, check_vma=False)
```
